32 devices in a mesh: sp: 8 (over z, y), tp: 4 (over x, core).
Axes of the slice: x: 2, y: 2, z: 4, core: 2. Of those that a mesh axis runs over, the one named last changes fastest.
Arguments:
- inputs: bfloat16 [4096, 4096], P('sp', 'tp'), may hold values from -24 to 24
- length: int32 [1], replicated, may hold values from 2049 to 4096
- win_query: bfloat16 [4096, 1536], P(None, 'tp'), may hold values from -8 to 8
- win_key: bfloat16 [4096, 512], P(None, 'tp'), may hold values from -8 to 8
- win_value: bfloat16 [4096, 512], P(None, 'tp'), may hold values from -1.5 to 1.5
- sink_logit: float32 [24], P('tp'), may hold values from 4 to 8
- diff_query: bfloat16 [4096, 1024], P(None, 'tp'), may hold values from -8 to 8
- diff_key: bfloat16 [4096, 1024], P(None, 'tp'), may hold values from -8 to 8
- diff_value: bfloat16 [4096, 1024], P(None, 'tp'), may hold values from -0.09375 to 0.09375
- mix_lambda: float32 [16], P('tp'), may hold values from 0.3 to 0.8
- head_gain: float32 [64], replicated, may hold values from 0.1 to 1.9
- win_out: bfloat16 [1536, 4096], P('tp'), may hold values from -0.125 to 0.125
- diff_out: bfloat16 [1024, 4096], P('tp'), may hold values from -0.125 to 0.125
Outputs:
- merged_out: bfloat16 [4096, 4096], P(('sp', 'tp'))
The draws below stay inside these ranges and needn't reach their ends.
All inputs are finite; a program needn't handle non-finite values.
Results may differ from the reference program's by a relative error of at most 0.015.
Values may be sent and summed in bfloat16 or wider, within the bound.
No kernel may reach another device: no remote copies, remote signals or barrier semaphores. Data moves between devices by JAX's collectives and lax.ppermute only.
A program may use at most 128 MiB of HBM per device.

```python
import jax
import jax.numpy as jnp
from jax import lax

D = 4096
HEAD = 64
DQK = 32
WKV = 8
GROUP = 3
WQH = 24
DH = 16
WINDOW = 128
TOKENS = 4096
N_TP = 4


def clipped(key, shape):
    return jnp.clip(jax.random.normal(key, shape, jnp.float32), -6.0, 6.0)


def window_pair(key):
    key_weight = clipped(jax.random.fold_in(key, 101), (D, WKV * HEAD)) * D ** (-0.5)
    noise_part = clipped(jax.random.fold_in(key, 102), (D, WKV * GROUP * HEAD)) * D ** (-0.5)
    query_weight = noise_part
    return (query_weight, key_weight)


def diff_pair(key):
    key_weight = clipped(jax.random.fold_in(key, 201), (D, DH * 2 * DQK)) * D ** (-0.5)
    noise_part = clipped(jax.random.fold_in(key, 202), (D, DH * 2 * DQK)) * (3.0 / D) ** 0.5
    query_weight = noise_part
    return (query_weight, key_weight)


def draw_inputs(key, part):
    base_rows = clipped(jax.random.fold_in(key, 301), (TOKENS, D))
    return base_rows.astype(jnp.bfloat16)


def draw_win_query(key, part):
    return window_pair(key)[0].astype(jnp.bfloat16)


def draw_win_key(key, part):
    return window_pair(key)[1].astype(jnp.bfloat16)


def draw_diff_query(key, part):
    return diff_pair(key)[0].astype(jnp.bfloat16)


def draw_diff_key(key, part):
    return diff_pair(key)[1].astype(jnp.bfloat16)


def block_scale(key, dims, cuts, low, top_value):
    gain, own = 1.0, jax.random.fold_in(key, 6)
    for dim, shards_of in cuts:
        steps = jnp.exp(jax.random.uniform(jax.random.fold_in(own, dim), (shards_of,), jnp.float32, low / len(cuts), top_value / len(cuts)))
        gain = gain * jnp.repeat(steps, dims[dim] // shards_of).reshape([-1 if axis == dim else 1 for axis in range(len(dims))])
    return gain


def gaussian(stream_key, shape, deviation, most, pieces=(), dtype=jnp.bfloat16):
    array = jax.random.normal(stream_key, shape, jnp.float32) * deviation
    if len(pieces) > 0:
        array = block_scale(stream_key, shape, pieces, -0.22, 0.18) * array
    return jnp.clip(array, min=-most, max=most).astype(dtype)


def setup_inputs(seed: int = 0) -> dict:
    splits = jax.random.split(jax.random.key(seed), 14)
    return {
        "inputs": draw_inputs(jax.random.fold_in(splits[13], 71), 0),
        "length": jax.random.randint(splits[1], (1,), TOKENS // 2 + 1, TOKENS + 1).astype(jnp.int32),
        "win_query": draw_win_query(jax.random.fold_in(splits[13], 71), 0),
        "win_key": draw_win_key(jax.random.fold_in(splits[13], 71), 0),
        "win_value": gaussian(splits[4], (D, WKV * HEAD), (max(D // 256, 1)) ** -0.5, 1.5, ((1, 4),)),
        "sink_logit": jnp.clip(4.0 + 4.0 * jax.random.uniform(splits[5], (WQH,), jnp.float32) ** block_scale(splits[5], (WQH,), ((0, 4),), -0.2, 0.2), 4.0, 8.0),
        "diff_query": draw_diff_query(jax.random.fold_in(splits[13], 71), 0),
        "diff_key": draw_diff_key(jax.random.fold_in(splits[13], 71), 0),
        "diff_value": gaussian(splits[8], (D, DH * HEAD), D ** -0.5, 0.09375, ((1, 4),)),
        "mix_lambda": jnp.clip(0.3 + 0.5 * jax.random.uniform(splits[9], (DH,), jnp.float32) ** block_scale(splits[9], (DH,), ((0, 4),), -0.2, 0.2), 0.3, 0.8),
        "head_gain": jnp.clip(1.0 + 0.18 * jax.random.normal(splits[10], (HEAD,), jnp.float32), 0.1, 1.9),
        "win_out": gaussian(splits[11], (WQH * HEAD, D), ((WQH + DH) * HEAD) ** -0.5, 0.125, ((0, 4),)),
        "diff_out": gaussian(splits[12], (DH * HEAD, D), ((WQH + DH) * HEAD) ** -0.5, 0.125, ((0, 4),)),
    }


epsilon = 1e-06
masked_score = -1e+30

def window_attention(win_q, win_k, win_v, sink_logit, live_count):
    queries = win_q.reshape(TOKENS, WKV, GROUP, HEAD)
    padded_k = jnp.pad(win_k.reshape(TOKENS, WKV, HEAD), ((WINDOW, WINDOW), (0, 0), (0, 0)))
    padded_v = jnp.pad(win_v.reshape(TOKENS, WKV, HEAD), ((WINDOW, WINDOW), (0, 0), (0, 0)))
    sink_table = sink_logit.reshape(WKV, GROUP)
    block_rows = 512
    block_count = TOKENS // block_rows

    def one_block(block_index):
        first_row = (block_index * block_rows).astype(jnp.int32)
        query_slab = lax.dynamic_slice_in_dim(queries, first_row, block_rows, 0).astype(jnp.float32)
        key_slab = lax.dynamic_slice_in_dim(padded_k, first_row, block_rows + 2 * WINDOW, 0).astype(jnp.float32)
        value_slab = lax.dynamic_slice_in_dim(padded_v, first_row, block_rows + 2 * WINDOW, 0).astype(jnp.float32)
        query_pos = first_row + jnp.arange(block_rows).astype(jnp.int32)
        key_pos = first_row - WINDOW + jnp.arange(block_rows + 2 * WINDOW).astype(jnp.int32)
        allowed = (jnp.abs(query_pos[:, None] - key_pos[None, :]) <= WINDOW) & (key_pos[None, :] >= 0) & (key_pos[None, :] < live_count)
        scores = jnp.einsum('qhgd,khd->hgqk', query_slab, key_slab) * HEAD ** (-0.5)
        scores = jnp.where(allowed[None, None], scores, masked_score)
        row_max = jnp.maximum(lax.optimization_barrier(jnp.max(scores, axis=-1)), sink_table[:, :, None])
        exponent = jnp.where(allowed[None, None], jnp.exp(scores - row_max[..., None]), 0.0)
        denominator = lax.optimization_barrier(jnp.sum(exponent, axis=-1)) + jnp.exp(sink_table[:, :, None] - row_max)
        weights_low = lax.optimization_barrier(exponent.astype(jnp.bfloat16)).astype(jnp.float32)
        result = jnp.einsum('hgqk,khd->qhgd', weights_low, value_slab) / jnp.transpose(denominator, (2, 0, 1))[..., None]
        result = jnp.where((query_pos < live_count)[:, None, None, None], result, 0.0)
        return result.reshape(block_rows, WQH * HEAD).astype(jnp.bfloat16)
    return lax.map(one_block, jnp.arange(block_count)).reshape(TOKENS, WQH * HEAD)

def diff_attention(diff_q, diff_k, diff_v, mix_lambda, head_gain, live_count):
    queries = diff_q.reshape(TOKENS, DH, 2, DQK)
    key_all = diff_k.reshape(TOKENS, DH, 2, DQK)
    value_all = diff_v.reshape(TOKENS, DH, HEAD)
    key_live = jnp.arange(TOKENS).astype(jnp.int32) < live_count
    block_rows = 512
    block_count = TOKENS // block_rows

    def one_head(head_index):
        query_head = lax.dynamic_index_in_dim(queries, head_index, 1, keepdims=False).astype(jnp.float32)
        key_head = lax.dynamic_index_in_dim(key_all, head_index, 1, keepdims=False).astype(jnp.float32)
        value_head = lax.dynamic_index_in_dim(value_all, head_index, 1, keepdims=False).astype(jnp.float32)
        mix_weight = lax.dynamic_index_in_dim(mix_lambda, head_index, 0, keepdims=False)

        def one_block(block_index):
            first_row = (block_index * block_rows).astype(jnp.int32)
            query_slab = lax.dynamic_slice_in_dim(query_head, first_row, block_rows, 0)
            scores = jnp.einsum('qmd,kmd->mqk', query_slab, key_head) * DQK ** (-0.5)
            scores = jnp.where(key_live[None, None], scores, masked_score)
            row_max = lax.optimization_barrier(jnp.max(scores, axis=-1, keepdims=True))
            exponent = jnp.where(key_live[None, None], jnp.exp(scores - row_max), 0.0)
            total_sum = lax.optimization_barrier(jnp.sum(exponent, axis=-1))
            weights_low = lax.optimization_barrier(exponent.astype(jnp.bfloat16)).astype(jnp.float32)
            map_rows = jnp.einsum('mqk,kd->mqd', weights_low, value_head) / total_sum[..., None]
            mixed_rows = map_rows[0] - mix_weight * map_rows[1]
            normed = mixed_rows * lax.rsqrt(lax.optimization_barrier(jnp.mean(mixed_rows * mixed_rows, axis=-1, keepdims=True)) + epsilon) * head_gain
            query_pos = first_row + jnp.arange(block_rows).astype(jnp.int32)
            return jnp.where((query_pos < live_count)[:, None], normed, 0.0)
        return lax.map(one_block, jnp.arange(block_count)).reshape(TOKENS, HEAD)
    result = lax.map(one_head, jnp.arange(DH))
    return jnp.transpose(result, (1, 0, 2)).reshape(TOKENS, DH * HEAD).astype(jnp.bfloat16)

def reference(inputs, length, win_query, win_key, win_value, sink_logit, diff_query, diff_key, diff_value, mix_lambda, head_gain, win_out, diff_out):
    live_count = length[0]

    def project(weight):
        return jnp.dot(inputs, weight, preferred_element_type=jnp.float32).astype(jnp.bfloat16)
    win_rows = window_attention(project(win_query), project(win_key), project(win_value), sink_logit, live_count)
    diff_rows = diff_attention(project(diff_query), project(diff_key), project(diff_value), mix_lambda, head_gain, live_count)
    win_cols = WQH // N_TP * HEAD
    diff_cols = DH // N_TP * HEAD
    merged = jnp.zeros((TOKENS, D), jnp.float32)
    for group_index in range(N_TP):
        partial_value = jnp.dot(win_rows[:, group_index * win_cols:(group_index + 1) * win_cols], win_out[group_index * win_cols:(group_index + 1) * win_cols], preferred_element_type=jnp.float32)
        partial_value = partial_value + jnp.dot(diff_rows[:, group_index * diff_cols:(group_index + 1) * diff_cols], diff_out[group_index * diff_cols:(group_index + 1) * diff_cols], preferred_element_type=jnp.float32)
        partial_value = lax.optimization_barrier(partial_value.astype(jnp.bfloat16)).astype(jnp.float32)
        merged = merged + partial_value
    return merged.astype(jnp.bfloat16)
```

```python
import functools
import math

import jax
import jax.numpy as jnp
from jax import lax
from jax.experimental import pallas as pl
from jax.experimental.pallas import tpu as pltpu
from jax.sharding import PartitionSpec as P

HEAD = 64
DQK = 32
GROUP = 3
WINDOW = 128

epsilon = 1e-06
masked_score = -1e30
LOG2E = math.log2(math.e)
SAFE_BOUND = 90.0


def whole(shape):
    return pl.BlockSpec(shape, lambda *_: (0,) * len(shape))


def smem():
    return pl.BlockSpec(memory_space=pltpu.SMEM)


def flip(axis, bits):
    return [(i, i ^ bits) for i in range(lax.axis_size(axis))]


def add_slice(x, weight_refs, acc_ref):
    weight = jnp.concatenate([ref[...] for ref in weight_refs], axis=1)
    acc_ref[...] += jnp.dot(x, weight, preferred_element_type=jnp.float32)


def first_kernel(steps, idx_ref, own_ref, sib_ref, *refs):
    acc_ref = refs[-1]
    j = pl.program_id(0)

    @pl.when(j == 0)
    def _():
        acc_ref[...] = jnp.zeros_like(acc_ref)

    x = jnp.where(j < steps, own_ref[...], sib_ref[...])
    add_slice(x, refs[:-1], acc_ref)


def project_near(own, sib, weights, index, steps):
    rows, depth = own.shape
    block = depth // steps
    width = sum(w.shape[1] for w in weights)

    def at_weight(j, idx):
        return (idx[j // steps] * steps + j % steps, 0)

    grid_spec = pltpu.PrefetchScalarGridSpec(
        num_scalar_prefetch=1,
        grid=(2 * steps,),
        in_specs=[
            pl.BlockSpec((rows, block), lambda j, idx: (0, jnp.minimum(j, steps - 1))),
            pl.BlockSpec((rows, block), lambda j, idx: (0, jnp.maximum(j - steps, 0))),
        ]
        + [pl.BlockSpec((block, w.shape[1]), at_weight) for w in weights],
        out_specs=pl.BlockSpec((rows, width), lambda j, idx: (0, 0)),
    )
    return pl.pallas_call(
        functools.partial(first_kernel, steps),
        grid_spec=grid_spec,
        out_shape=jax.ShapeDtypeStruct((rows, width), jnp.float32),
        compiler_params=pltpu.CompilerParams(dimension_semantics=("arbitrary",)),
        name="project_near",
    )(index, own, sib, *weights)


def last_kernel(steps, count, heads, idx_ref, acc_in_ref, *refs):
    xs = refs[:count]
    weight_refs = refs[count : count + 6]
    qt_ref, kv_ref, buf_ref, acc_ref = refs[count + 6 :]
    j = pl.program_id(0)

    @pl.when(j == 0)
    def _():
        acc_ref[...] = acc_in_ref[...]

    x = xs[0][...]
    for i in range(1, count):
        x = jnp.where(j < i * steps, x, xs[i][...])
    add_slice(x, weight_refs, acc_ref)

    @pl.when(j == count * steps - 1)
    def _():
        rows = acc_ref.shape[0]
        sizes = [ref.shape[1] for ref in weight_refs]
        starts = [sum(sizes[:i]) for i in range(6)]
        here = idx_ref[count]

        def part(i, low=0, size=None):
            begin = starts[i] + low
            return acc_ref[:, begin : begin + (sizes[i] if size is None else size)]

        win_q = part(0) * (LOG2E * HEAD ** (-0.5))
        qt_ref[...] = jnp.transpose(win_q).astype(jnp.bfloat16)
        kv_ref[...] = jnp.concatenate([part(1), part(2)], axis=1).astype(jnp.bfloat16)
        for h in range(heads):
            q = part(3, h * HEAD, HEAD) * (LOG2E * DQK ** (-0.5))
            k = part(4, h * HEAD, HEAD)
            v = part(5, h * HEAD, HEAD)
            slot = h ^ here
            buf_ref[slot, 0:rows, :] = jnp.concatenate([k, v], axis=1).astype(jnp.bfloat16)
            pair = jnp.concatenate([q[: rows // 2], q[rows // 2 :]], axis=1)
            buf_ref[slot, rows : rows + rows // 2, :] = pair.astype(jnp.bfloat16)


def project_far(acc, chunk, rows, xs, weights, index, steps, heads):
    depth = xs[0].shape[1]
    block = depth // steps
    count = len(xs)
    width = acc.shape[1]

    def at_weight(j, idx):
        return (idx[j // steps] * steps + j % steps, 0)

    def at_x(i):
        return lambda j, idx: (0, jnp.clip(j - i * steps, 0, steps - 1))

    kv_width = weights[1].shape[1] + weights[2].shape[1]
    q_width = weights[0].shape[1]
    grid_spec = pltpu.PrefetchScalarGridSpec(
        num_scalar_prefetch=1,
        grid=(count * steps,),
        in_specs=[pl.BlockSpec((rows, width), lambda j, idx: (chunk, 0))]
        + [pl.BlockSpec((rows, block), at_x(i)) for i in range(count)]
        + [pl.BlockSpec((block, w.shape[1]), at_weight) for w in weights],
        out_specs=[
            whole((q_width, rows)),
            whole((rows, kv_width)),
            whole((heads, rows + rows // 2, 2 * HEAD)),
        ],
        scratch_shapes=[pltpu.VMEM((rows, width), jnp.float32)],
    )
    return pl.pallas_call(
        functools.partial(last_kernel, steps, count, heads),
        grid_spec=grid_spec,
        out_shape=[
            jax.ShapeDtypeStruct((q_width, rows), jnp.bfloat16),
            jax.ShapeDtypeStruct((rows, kv_width), jnp.bfloat16),
            jax.ShapeDtypeStruct((heads, rows + rows // 2, 2 * HEAD), jnp.bfloat16),
        ],
        compiler_params=pltpu.CompilerParams(dimension_semantics=("arbitrary",)),
        name="project_far",
    )(index, acc, *xs, *weights)


def window_kernel(chunks, rows, kv_local, scal_ref, sink_ref, *refs):
    q_refs = refs[:chunks]
    kv_refs = refs[chunks : 2 * chunks]
    low_ref, high_ref, out_ref, keys, values_t = refs[2 * chunks :]
    here, live = scal_ref[0], scal_ref[1]
    span = rows + 2 * WINDOW
    size = rows // chunks
    keys[0:WINDOW, :] = low_ref[...]
    for c in range(chunks):
        keys[WINDOW + c * size : WINDOW + (c + 1) * size, :] = kv_refs[c][...]
    keys[WINDOW + rows : span, :] = high_ref[...]
    k_width = kv_local * HEAD
    turned = jnp.transpose(keys[:, k_width:].astype(jnp.float32)).astype(jnp.bfloat16)
    tail = (lax.broadcasted_iota(jnp.int32, (16, span), 0) == 0).astype(jnp.bfloat16)
    for h in range(kv_local):
        values_t[h, 0:HEAD, :] = turned[h * HEAD : (h + 1) * HEAD]
        values_t[h, HEAD : HEAD + 16, :] = tail
    step = 128
    for b in range(rows // step):
        first = here * rows + b * step

        @pl.when(first >= live)
        def _():
            out_ref[:, b * step : (b + 1) * step] = jnp.zeros(
                (out_ref.shape[0], step), jnp.bfloat16
            )

        @pl.when(first < live)
        def _():
            wide = step + 2 * WINDOW
            c, at = (b * step) // size, (b * step) % size
            key_at = lax.broadcasted_iota(jnp.int32, (wide, step), 0)
            query_at = lax.broadcasted_iota(jnp.int32, (wide, step), 1)
            key_pos = first - WINDOW + key_at
            gap = key_at - WINDOW - query_at
            allowed = (
                (gap <= WINDOW) & (gap >= -WINDOW) & (key_pos >= 0) & (key_pos < live)
            )
            live_row = (
                first + lax.broadcasted_iota(jnp.int32, (1, step), 1)
            ) < live
            for h in range(kv_local):
                key_block = keys[b * step : b * step + wide, h * HEAD : (h + 1) * HEAD]
                value_block = values_t[h, :, b * step : b * step + wide]
                for g in range(GROUP):
                    head = h * GROUP + g
                    q = q_refs[c][head * HEAD : (head + 1) * HEAD, at : at + step]
                    s = jnp.dot(key_block, q, preferred_element_type=jnp.float32)
                    s = jnp.where(allowed, s, masked_score)
                    sink = sink_ref[head] * LOG2E
                    top = jnp.maximum(jnp.max(s, axis=0, keepdims=True), sink)
                    e = jnp.exp2(s - top).astype(jnp.bfloat16)
                    mixed = jnp.dot(value_block, e, preferred_element_type=jnp.float32)
                    total = mixed[HEAD : HEAD + 1] + jnp.exp2(sink - top)
                    result = jnp.where(live_row, mixed[0:HEAD] / total, 0.0)
                    out_ref[head * HEAD : (head + 1) * HEAD, b * step : (b + 1) * step] = (
                        result.astype(jnp.bfloat16)
                    )


def window_part(scal, sink_logit, q_parts, kv_parts, low, high):
    chunks = len(q_parts)
    q_width, size = q_parts[0].shape
    kv_width = kv_parts[0].shape[1]
    rows = size * chunks
    kv_local = kv_width // (2 * HEAD)
    operands = (*q_parts, *kv_parts, low, high)
    return pl.pallas_call(
        functools.partial(window_kernel, chunks, rows, kv_local),
        in_specs=[smem(), smem()] + [whole(a.shape) for a in operands],
        out_specs=whole((q_width, rows)),
        out_shape=jax.ShapeDtypeStruct((q_width, rows), jnp.bfloat16),
        scratch_shapes=[
            pltpu.VMEM((rows + 2 * WINDOW, kv_width), jnp.bfloat16),
            pltpu.VMEM((kv_local, HEAD + 16, rows + 2 * WINDOW), jnp.bfloat16),
        ],
        grid=(1,),
        name="window",
    )(scal, sink_logit, *operands)


def diff_kernel(chunks, rows, parts, count, scal_ref, lam_ref, gain_ref, *refs):
    block_refs = refs[: chunks * count]
    out_ref, keys, values_t, queries, weighted, running = refs[chunks * count :]
    here, live = scal_ref[0], scal_ref[1]
    heads = count // parts
    size = rows // chunks
    total = rows * count
    step = 512
    pair = 2 * size

    top_key = jnp.zeros((1, 2 * HEAD), jnp.float32)
    queries[...] = jnp.zeros_like(queries)
    for c in range(chunks):
        for d in range(count):
            ref = block_refs[c * count + d]
            at = pl.multiple_of((here ^ d) * rows + c * size, size)
            block = ref[0:size, :]
            keys[pl.ds(at, size), :] = block
            wide = block.astype(jnp.float32)
            top_key = jnp.maximum(top_key, jnp.max(jnp.abs(wide), axis=0, keepdims=True))
            values_t[0:HEAD, pl.ds(at, size)] = jnp.transpose(wide)[HEAD:].astype(jnp.bfloat16)
            if d % parts == 0:
                half = size // 2
                turned = jnp.transpose(ref[size : size + half, :].astype(jnp.float32))
                turned = jnp.concatenate([turned[0:HEAD], turned[HEAD:]], axis=1)
                turned = turned.astype(jnp.bfloat16)
                tile = c * heads + d // parts
                queries[tile, 0:DQK, 0:size] = turned[0:DQK]
                queries[tile, DQK : 2 * DQK, size:pair] = turned[DQK:]
    values_t[HEAD : HEAD + 16, :] = (
        lax.broadcasted_iota(jnp.int32, (16, total), 0) == 0
    ).astype(jnp.bfloat16)
    limit = jnp.transpose(jnp.broadcast_to(top_key, (8, 2 * HEAD)))[:, 0:1]

    full = live // step
    left = live - full * step

    def tile_body(tile, carry):
        c, zd = tile // heads, tile % heads
        first = (here ^ (zd * parts)) * rows + c * size

        @pl.when(first >= live)
        def _():
            out_ref[tile] = jnp.zeros(out_ref.shape[1:], out_ref.dtype)

        @pl.when(first < live)
        def _():
            q = queries[tile]
            bound = jnp.max(jnp.sum(jnp.abs(q.astype(jnp.float32)) * limit, axis=0, keepdims=True))
            safe = bound < SAFE_BOUND

            def scores(j):
                at = pl.multiple_of(j * step, step)
                return jnp.dot(keys[pl.ds(at, step), :], q, preferred_element_type=jnp.float32)

            def values(j):
                return values_t[:, pl.ds(pl.multiple_of(j * step, step), step)]

            def inside(shape):
                return lax.broadcasted_iota(jnp.int32, shape, 0) < left

            weighted[...] = jnp.zeros_like(weighted)

            @pl.when(safe)
            def _():
                def one(j, carry):
                    e = jnp.exp2(scores(j)).astype(jnp.bfloat16)
                    weighted[...] += jnp.dot(values(j), e, preferred_element_type=jnp.float32)
                    return carry

                lax.fori_loop(0, full, one, 0)

                @pl.when(left > 0)
                def _():
                    s = scores(full)
                    e = jnp.where(inside(s.shape), jnp.exp2(s), 0.0).astype(jnp.bfloat16)
                    weighted[...] += jnp.dot(values(full), e, preferred_element_type=jnp.float32)

            @pl.when(jnp.logical_not(safe))
            def _():
                running[...] = jnp.full_like(running, masked_score)

                def add(j, s):
                    old = running[...]
                    new = jnp.maximum(old, jnp.max(s, axis=0, keepdims=True))
                    e = jnp.exp2(s - new).astype(jnp.bfloat16)
                    weighted[...] = weighted[...] * jnp.exp2(old - new) + jnp.dot(
                        values(j), e, preferred_element_type=jnp.float32
                    )
                    running[...] = new

                def one(j, carry):
                    add(j, scores(j))
                    return carry

                lax.fori_loop(0, full, one, 0)

                @pl.when(left > 0)
                def _():
                    s = scores(full)
                    add(full, jnp.where(inside(s.shape), s, masked_score))

            maps = weighted[0:HEAD, :] / weighted[HEAD : HEAD + 1, :]
            mix = maps[:, 0:size] - lam_ref[here // parts] * maps[:, size:pair]
            normed = mix * lax.rsqrt(jnp.mean(mix * mix, axis=0, keepdims=True) + epsilon)
            normed = normed * gain_ref[...]
            position = first + lax.broadcasted_iota(jnp.int32, (1, size), 1)
            out_ref[tile] = jnp.where(position < live, normed, 0.0).astype(jnp.bfloat16)

        return carry

    lax.fori_loop(0, chunks * heads, tile_body, 0)


def diff_part(scal, mix_lambda, gain, blocks, chunks, rows, parts):
    count = len(blocks) // chunks
    heads = count // parts
    size = rows // chunks
    return pl.pallas_call(
        functools.partial(diff_kernel, chunks, rows, parts, count),
        in_specs=[smem(), smem(), whole(gain.shape)] + [whole(a.shape) for a in blocks],
        out_specs=whole((chunks * heads, HEAD, size)),
        out_shape=jax.ShapeDtypeStruct((chunks * heads, HEAD, size), jnp.bfloat16),
        scratch_shapes=[
            pltpu.VMEM((rows * count, 2 * HEAD), jnp.bfloat16),
            pltpu.VMEM((HEAD + 16, rows * count), jnp.bfloat16),
            pltpu.VMEM((chunks * heads, 2 * HEAD, 2 * size), jnp.bfloat16),
            pltpu.VMEM((HEAD + 16, 2 * size), jnp.float32),
            pltpu.VMEM((1, 2 * size), jnp.float32),
        ],
        grid=(1,),
        name="differential",
    )(scal, mix_lambda, gain, *blocks)


def out_kernel(heads, scal_ref, win_ref, *refs):
    diff_refs = refs[:heads]
    win_w_ref, diff_w_ref, out_ref, stacked = refs[heads:]
    chunk, here, core = scal_ref[0], scal_ref[1], scal_ref[2]
    size = stacked.shape[0]
    half = size // 2
    win_width = win_ref.shape[0]

    @pl.when(pl.program_id(0) == 0)
    def _():
        at = pl.multiple_of(chunk * size, size)
        turned = jnp.transpose(win_ref[:, pl.ds(at, size)].astype(jnp.float32))
        stacked[:, 0:win_width] = turned.astype(jnp.bfloat16)
        pieces = []
        for h in range(heads):
            piece = diff_refs[0][chunk]
            for d in range(1, heads):
                piece = jnp.where((here ^ d) == h, diff_refs[d][chunk], piece)
            pieces.append(piece)
        turned = jnp.transpose(jnp.concatenate(pieces, axis=0).astype(jnp.float32))
        stacked[:, win_width:] = turned.astype(jnp.bfloat16)

    weight = jnp.concatenate([win_w_ref[...], diff_w_ref[...]], axis=0)
    partial = jnp.dot(stacked[...], weight, preferred_element_type=jnp.float32)
    partial = partial.astype(jnp.bfloat16)
    out_ref[core] = partial[0:half]
    out_ref[1 - core] = partial[half:]


def out_part(scal, win_t, diffs, win_out, diff_out, begin, width, block, size):
    heads = len(diffs)
    depth = win_out.shape[0] + diff_out.shape[0]
    return pl.pallas_call(
        functools.partial(out_kernel, heads),
        in_specs=[smem(), whole(win_t.shape)]
        + [whole(a.shape) for a in diffs]
        + [
            pl.BlockSpec((w.shape[0], block), lambda j: (0, begin // block + j))
            for w in (win_out, diff_out)
        ],
        out_specs=pl.BlockSpec((2, size // 2, block), lambda j: (0, 0, j)),
        out_shape=jax.ShapeDtypeStruct((2, size // 2, width), jnp.bfloat16),
        scratch_shapes=[pltpu.VMEM((size, depth), jnp.bfloat16)],
        grid=(width // block,),
        compiler_params=pltpu.CompilerParams(dimension_semantics=("arbitrary",)),
        name="project_out",
    )(scal, win_t, *diffs, win_out, diff_out)


def body(
    inputs,
    length,
    win_query,
    win_key,
    win_value,
    sink_logit,
    diff_query,
    diff_key,
    diff_value,
    mix_lambda,
    head_gain,
    win_out,
    diff_out,
):
    rows = inputs.shape[0]
    sp, tp = lax.axis_size("sp"), lax.axis_size("tp")
    chips = tp // 2
    size = rows // chips
    heads = mix_lambda.shape[0]
    parts = sp // heads
    here, me = lax.axis_index("sp"), lax.axis_index("tp")
    chip, core = me // 2, me % 2
    weights = (win_query, win_key, win_value, diff_query, diff_key, diff_value)
    steps = 2

    pieces = [inputs[c * size : (c + 1) * size] for c in range(chips)]
    far = [
        [lax.ppermute(pieces[c], "tp", flip("tp", 2 * o)) for o in range(1, chips)]
        for c in range(chips)
    ]
    sib = lax.ppermute(inputs, "tp", flip("tp", 1))
    near_index = jnp.stack([me, me ^ 1]).astype(jnp.int32)
    acc = project_near(inputs, sib, weights, near_index, steps)
    order = [me ^ (2 * o + k) for o in range(1, chips) for k in range(2)]
    far_index = jnp.stack(order + [here // parts]).astype(jnp.int32)
    q_parts, kv_parts, bufs = [], [], []
    for c in range(chips):
        xs = []
        for piece in far[c]:
            xs += [piece, lax.ppermute(piece, "tp", flip("tp", 1))]
        q_t, kv, buf = project_far(acc, c, size, xs, weights, far_index, steps, heads)
        q_parts.append(q_t)
        kv_parts.append(kv)
        bufs.append(buf)

    blocks = []
    for c in range(chips):
        for d in range(sp):
            block = bufs[c][d // parts]
            if d % parts:
                block = block[:size]
            blocks.append(lax.ppermute(block, "sp", flip("sp", d)) if d else block)

    up = [(i, i + 1) for i in range(sp - 1)]
    down = [(i + 1, i) for i in range(sp - 1)]
    low = lax.ppermute(kv_parts[-1][size - WINDOW :], "sp", up)
    high = lax.ppermute(kv_parts[0][:WINDOW], "sp", down)
    scal = jnp.stack([here, length[0]]).astype(jnp.int32)
    win_t = window_part(scal, sink_logit, q_parts, kv_parts, low, high)

    gain = head_gain.reshape(HEAD, 1)
    mixed = diff_part(scal, mix_lambda, gain, blocks, chips, rows, parts)
    mixed = mixed.reshape(chips, heads, HEAD, size)
    diffs = [mixed[:, 0]]
    for d in range(1, heads):
        diffs.append(lax.ppermute(mixed[:, d], "sp", flip("sp", d * parts)))

    width = win_out.shape[1]
    cut = 4
    head_index = here // parts

    def project(o, begin, span):
        where = jnp.stack([chip ^ o, head_index, core]).astype(jnp.int32)
        return out_part(where, win_t, diffs, win_out, diff_out, begin, span, span, size)

    def add(*values):
        return functools.reduce(lambda a, b: a + b, [v.astype(jnp.float32) for v in values])

    arrived = []
    span = width // cut
    for i in range(cut):
        crossed = []
        for o in range(1, chips):
            both = project(o, i * span, span)
            other = lax.ppermute(both[1], "tp", flip("tp", 1))
            pair = add(both[0], other).astype(jnp.bfloat16)
            crossed.append(lax.ppermute(pair, "tp", flip("tp", 2 * o)))
        arrived.append(crossed)
    outs = []
    for i in range(cut):
        both = project(0, i * span, span)
        other = lax.ppermute(both[1], "tp", flip("tp", 1))
        outs.append(add(both[0], other, *arrived[i]).astype(jnp.bfloat16))
    return jnp.concatenate(outs, axis=1)


def solution(mesh):
    placed = (
        P("sp", "tp"),
        P(),
        P(None, "tp"),
        P(None, "tp"),
        P(None, "tp"),
        P("tp"),
        P(None, "tp"),
        P(None, "tp"),
        P(None, "tp"),
        P("tp"),
        P(),
        P("tp", None),
        P("tp", None),
    )
    return jax.shard_map(
        body, mesh=mesh, in_specs=placed, out_specs=P(("sp", "tp"), None), check_vma=False
    )
```

```python
import functools
import math

import jax
import jax.numpy as jnp
from jax import lax
from jax.experimental import pallas as pl
from jax.experimental.pallas import tpu as pltpu
from jax.sharding import PartitionSpec as P

HEAD = 64
DQK = 32
GROUP = 3
WINDOW = 128

epsilon = 1e-06
masked_score = -1e30
LOG2E = math.log2(math.e)
SAFE_BOUND = 90.0


def whole(shape):
    return pl.BlockSpec(shape, lambda *_: (0,) * len(shape))


def smem():
    return pl.BlockSpec(memory_space=pltpu.SMEM)


def cost(flops, bytes_accessed=0, transcendentals=0):
    return pl.CostEstimate(
        flops=flops, bytes_accessed=bytes_accessed, transcendentals=transcendentals
    )


def flip(axis, bits):
    return [(i, i ^ bits) for i in range(lax.axis_size(axis))]


def add_slice(x, weight_refs, acc_ref):
    weight = jnp.concatenate([ref[...] for ref in weight_refs], axis=1)
    acc_ref[...] += jnp.dot(x, weight, preferred_element_type=jnp.float32)


def first_kernel(steps, scal_ref, own_ref, sib_ref, *refs):
    acc_ref = refs[-1]
    j = pl.program_id(0)

    @pl.when(j == 0)
    def _():
        acc_ref[...] = jnp.zeros_like(acc_ref)

    x = jnp.where(j < steps, own_ref[...], sib_ref[...])
    add_slice(x, refs[:-1], acc_ref)


def project_near(own, sib, weights, scal, steps):
    rows, depth = own.shape
    block = depth // steps
    width = sum(w.shape[1] for w in weights)

    def at_weight(j, scal):
        return ((scal[2] ^ (j // steps)) * steps + j % steps, 0)

    grid_spec = pltpu.PrefetchScalarGridSpec(
        num_scalar_prefetch=1,
        grid=(2 * steps,),
        in_specs=[
            pl.BlockSpec((rows, block), lambda j, idx: (0, jnp.minimum(j, steps - 1))),
            pl.BlockSpec((rows, block), lambda j, idx: (0, jnp.maximum(j - steps, 0))),
        ]
        + [pl.BlockSpec((block, w.shape[1]), at_weight) for w in weights],
        out_specs=pl.BlockSpec((rows, width), lambda j, idx: (0, 0)),
    )
    return pl.pallas_call(
        functools.partial(first_kernel, steps),
        grid_spec=grid_spec,
        out_shape=jax.ShapeDtypeStruct((rows, width), jnp.float32),
        compiler_params=pltpu.CompilerParams(
            dimension_semantics=("arbitrary",), vmem_limit_bytes=24 << 20
        ),
        cost_estimate=cost(4 * rows * depth * width, 4 * depth * width),
        name="project_near",
    )(scal, own, sib, *weights)


def fetch_kernel(pieces, scal_ref, *refs):
    count = len(pieces)
    sources, targets, semaphores = refs[:count], refs[count : 2 * count], refs[2 * count]
    copies = []
    for source, target, slices in zip(sources, targets, pieces):
        depth = target.shape[0] // len(slices)
        for i, k in enumerate(slices):
            at = 0 if k is None else pl.multiple_of((scal_ref[2] ^ k) * depth, depth)
            copies.append(
                pltpu.make_async_copy(
                    source.at[pl.ds(at, depth), :],
                    target.at[pl.ds(i * depth, depth), :],
                    semaphores.at[len(copies)],
                )
            )
    for copy in copies:
        copy.start()
    for copy in copies:
        copy.wait()


def fetch(scal, arrays, slices, tp):
    shapes = [
        (a.shape[0] if slices == [None] else a.shape[0] // tp * len(slices), a.shape[1])
        for a in arrays
    ]
    return pl.pallas_call(
        functools.partial(fetch_kernel, [slices] * len(arrays)),
        in_specs=[smem()] + [pl.BlockSpec(memory_space=pl.ANY)] * len(arrays),
        out_specs=[pl.BlockSpec(memory_space=pltpu.VMEM)] * len(arrays),
        out_shape=[pltpu.VMEM(shape, jnp.bfloat16) for shape in shapes],
        scratch_shapes=[pltpu.SemaphoreType.DMA((len(arrays) * len(slices),))],
        compiler_params=pltpu.CompilerParams(vmem_limit_bytes=1 << 20),
        cost_estimate=cost(3 << 30),
        name="fetch",
    )(scal, *arrays)


def far_kernel(count, heads, parts, scal_ref, acc_ref, *refs):
    xs = refs[:count]
    weight_refs = refs[count : count + 6]
    qt_ref, kv_ref = refs[count + 6 : count + 8]
    slot_refs = refs[count + 8 : count + 8 + heads]
    buf_ref = refs[count + 8 + heads]
    rows, _ = xs[0].shape
    here = scal_ref[0] // parts

    def project(which):
        whole_x = jnp.concatenate([x[...] for x in xs], axis=1)
        weight = jnp.concatenate([weight_refs[i][...] for i in which], axis=1)
        low = sum(weight_refs[i].shape[1] for i in range(which[0]))
        span = weight.shape[1]
        total = acc_ref[:, low : low + span] + jnp.dot(
            whole_x, weight, preferred_element_type=jnp.float32
        )
        ends = [sum(weight_refs[i].shape[1] for i in which[:n]) for n in range(len(which) + 1)]
        return [total[:, a:b] for a, b in zip(ends[:-1], ends[1:])]

    win_q, win_k, win_v, diff_q, diff_k, diff_v = project(range(6))
    diff_q = diff_q * (LOG2E * DQK ** (-0.5))
    for h in range(heads):
        lanes = slice(h * HEAD, (h + 1) * HEAD)
        q, k, v = diff_q[:, lanes], diff_k[:, lanes], diff_v[:, lanes]
        buf_ref[h, 0:rows, :] = jnp.concatenate([k, v], axis=1).astype(jnp.bfloat16)
        pair = jnp.concatenate([q[: rows // 2], q[rows // 2 :]], axis=1)
        buf_ref[h, rows : rows + rows // 2, :] = pair.astype(jnp.bfloat16)
    for slot in range(heads):
        slot_refs[slot][...] = buf_ref[slot ^ here]
    qt_ref[...] = jnp.transpose(win_q * (LOG2E * HEAD ** (-0.5))).astype(jnp.bfloat16)
    kv_ref[...] = jnp.concatenate([win_k, win_v], axis=1).astype(jnp.bfloat16)


def project_far(acc, chunk, rows, xs, weights, scal, heads, parts):
    depth = xs[0].shape[1]
    count = len(xs)
    width = acc.shape[1]
    kv_width = weights[1].shape[1] + weights[2].shape[1]
    q_width = weights[0].shape[1]
    shapes = [(q_width, rows), (rows, kv_width)] + [(rows + rows // 2, 2 * HEAD)] * heads
    return pl.pallas_call(
        functools.partial(far_kernel, count, heads, parts),
        in_specs=[smem(), pl.BlockSpec((rows, width), lambda j: (chunk, 0))]
        + [whole((rows, depth))] * count
        + [pl.BlockSpec(memory_space=pltpu.VMEM)] * 6,
        out_specs=[whole(shape) for shape in shapes],
        out_shape=[jax.ShapeDtypeStruct(shape, jnp.bfloat16) for shape in shapes],
        scratch_shapes=[pltpu.VMEM((heads, rows + rows // 2, 2 * HEAD), jnp.bfloat16)],
        grid=(1,),
        compiler_params=pltpu.CompilerParams(vmem_limit_bytes=24 << 20),
        cost_estimate=cost(2 * count * rows * depth * width),
        name="project_far",
    )(scal, acc, *xs, *weights)


def window_kernel(chunks, rows, kv_local, scal_ref, sink_ref, *refs):
    q_refs = refs[:chunks]
    kv_refs = refs[chunks : 2 * chunks]
    low_ref, high_ref, rows_ref, keys, values_t, out_ref = refs[2 * chunks :]
    here, live = scal_ref[0], scal_ref[1]
    span = rows + 2 * WINDOW
    size = rows // chunks
    keys[0:WINDOW, :] = low_ref[...]
    for c in range(chunks):
        keys[WINDOW + c * size : WINDOW + (c + 1) * size, :] = kv_refs[c][...]
    keys[WINDOW + rows : span, :] = high_ref[...]
    k_width = kv_local * HEAD
    turned = jnp.transpose(keys[:, k_width:].astype(jnp.float32)).astype(jnp.bfloat16)
    tail = (lax.broadcasted_iota(jnp.int32, (16, span), 0) == 0).astype(jnp.bfloat16)
    for h in range(kv_local):
        values_t[h, 0:HEAD, :] = turned[h * HEAD : (h + 1) * HEAD]
        values_t[h, HEAD : HEAD + 16, :] = tail
    step = 128
    for b in range(rows // step):
        first = here * rows + b * step

        @pl.when(first >= live)
        def _():
            out_ref[:, b * step : (b + 1) * step] = jnp.zeros(
                (out_ref.shape[0], step), jnp.float32
            )

        @pl.when(first < live)
        def _():
            wide = step + 2 * WINDOW
            c, at = (b * step) // size, (b * step) % size
            key_at = lax.broadcasted_iota(jnp.int32, (wide, step), 0)
            query_at = lax.broadcasted_iota(jnp.int32, (wide, step), 1)
            key_pos = first - WINDOW + key_at
            gap = key_at - WINDOW - query_at
            allowed = (
                (gap <= WINDOW) & (gap >= -WINDOW) & (key_pos >= 0) & (key_pos < live)
            )
            live_row = (
                first + lax.broadcasted_iota(jnp.int32, (1, step), 1)
            ) < live
            for h in range(kv_local):
                key_block = keys[b * step : b * step + wide, h * HEAD : (h + 1) * HEAD]
                value_block = values_t[h, :, b * step : b * step + wide]
                for g in range(GROUP):
                    head = h * GROUP + g
                    q = q_refs[c][head * HEAD : (head + 1) * HEAD, at : at + step]
                    s = jnp.dot(key_block, q, preferred_element_type=jnp.float32)
                    s = jnp.where(allowed, s, masked_score)
                    sink = sink_ref[head] * LOG2E
                    top = jnp.maximum(jnp.max(s, axis=0, keepdims=True), sink)
                    e = jnp.exp2(s - top).astype(jnp.bfloat16)
                    mixed = jnp.dot(value_block, e, preferred_element_type=jnp.float32)
                    total = mixed[HEAD : HEAD + 1] + jnp.exp2(sink - top)
                    result = jnp.where(live_row, mixed[0:HEAD] / total, 0.0)
                    out_ref[head * HEAD : (head + 1) * HEAD, b * step : (b + 1) * step] = (
                        result
                    )

        block = out_ref[:, b * step : (b + 1) * step]
        rows_ref[b * step : (b + 1) * step, :] = jnp.transpose(block).astype(jnp.bfloat16)


def window_part(scal, sink_logit, q_parts, kv_parts, low, high):
    chunks = len(q_parts)
    q_width, size = q_parts[0].shape
    kv_width = kv_parts[0].shape[1]
    rows = size * chunks
    kv_local = kv_width // (2 * HEAD)
    operands = (*q_parts, *kv_parts, low, high)
    return pl.pallas_call(
        functools.partial(window_kernel, chunks, rows, kv_local),
        in_specs=[smem(), smem()] + [whole(a.shape) for a in operands],
        out_specs=whole((rows, q_width)),
        out_shape=jax.ShapeDtypeStruct((rows, q_width), jnp.bfloat16),
        scratch_shapes=[
            pltpu.VMEM((rows + 2 * WINDOW, kv_width), jnp.bfloat16),
            pltpu.VMEM((kv_local, HEAD + 16, rows + 2 * WINDOW), jnp.bfloat16),
            pltpu.VMEM((q_width, rows), jnp.float32),
        ],
        grid=(1,),
        compiler_params=pltpu.CompilerParams(vmem_limit_bytes=16 << 20),
        cost_estimate=cost(40 * q_width * rows * 384),
        name="window",
    )(scal, sink_logit, *operands)


def diff_kernel(chunks, rows, parts, count, scal_ref, lam_ref, gain_ref, *refs):
    heads = count // parts
    kv_refs = refs[: chunks * parts]
    q_refs = refs[chunks * parts : chunks * (parts + heads)]
    out_refs = refs[chunks * (parts + heads) : chunks * (parts + heads) + heads]
    out_ref, keys, values_t, queries, weighted, running = refs[-6:]
    here, live = scal_ref[0], scal_ref[1]
    size = rows // chunks
    total = rows * count
    step = 512
    pair = 2 * size

    top_key = jnp.zeros((1, 2 * HEAD), jnp.float32)
    queries[...] = jnp.zeros_like(queries)
    for c in range(chunks):
        for d in range(count):
            at = pl.multiple_of((here ^ d) * rows + c * size, size)
            block = kv_refs[c * parts + d % parts][d // parts]
            keys[pl.ds(at, size), :] = block
            wide = block.astype(jnp.float32)
            top_key = jnp.maximum(top_key, jnp.max(jnp.abs(wide), axis=0, keepdims=True))
            alive = (at + lax.broadcasted_iota(jnp.int32, (1, size), 1)) < live
            turned = jnp.where(alive, jnp.transpose(wide)[HEAD:], 0.0)
            values_t[0:HEAD, pl.ds(at, size)] = turned.astype(jnp.bfloat16)
            if d % parts == 0:
                half = size // 2
                pairs = q_refs[c * heads + d // parts][size : size + half, :]
                turned = jnp.transpose(pairs.astype(jnp.float32))
                turned = jnp.concatenate([turned[0:HEAD], turned[HEAD:]], axis=1)
                turned = turned.astype(jnp.bfloat16)
                tile = c * heads + d // parts
                queries[tile, 0:DQK, 0:size] = turned[0:DQK]
                queries[tile, DQK : 2 * DQK, size:pair] = turned[DQK:]
    counted = lax.broadcasted_iota(jnp.int32, (16, total), 0) == 0
    counted &= lax.broadcasted_iota(jnp.int32, (16, total), 1) < live
    values_t[HEAD : HEAD + 16, :] = counted.astype(jnp.bfloat16)
    limit = jnp.transpose(jnp.broadcast_to(top_key, (8, 2 * HEAD)))[:, 0:1]
    gain = jnp.transpose(jnp.broadcast_to(gain_ref[...], (8, HEAD)))[:, 0:1]

    full = live // step
    left = live - full * step

    def tile_body(tile, carry):
        c, zd = tile // heads, tile % heads
        first = (here ^ (zd * parts)) * rows + c * size

        @pl.when(first >= live)
        def _():
            out_ref[tile] = jnp.zeros(out_ref.shape[1:], out_ref.dtype)

        @pl.when(first < live)
        def _():
            q = queries[tile]
            bound = jnp.max(jnp.sum(jnp.abs(q.astype(jnp.float32)) * limit, axis=0, keepdims=True))
            safe = bound < SAFE_BOUND

            def scores(j):
                at = pl.multiple_of(j * step, step)
                return jnp.dot(keys[pl.ds(at, step), :], q, preferred_element_type=jnp.float32)

            def values(j):
                return values_t[:, pl.ds(pl.multiple_of(j * step, step), step)]

            def inside(shape):
                return lax.broadcasted_iota(jnp.int32, shape, 0) < left

            weighted[...] = jnp.zeros_like(weighted)

            @pl.when(safe)
            def _():
                def several(j, number):
                    raised = [jnp.exp2(scores(j + i)).astype(jnp.bfloat16) for i in range(number)]
                    added = [
                        jnp.dot(values(j + i), e, preferred_element_type=jnp.float32)
                        for i, e in enumerate(raised)
                    ]
                    weighted[...] += functools.reduce(lambda a, b: a + b, added)

                def one(j, carry):
                    several(4 * j, 4)
                    return carry

                pairs = (live + 2 * step - 1) // (2 * step)
                lax.fori_loop(0, pairs // 2, one, 0)

                @pl.when(pairs % 2 == 1)
                def _():
                    several(2 * (pairs - 1), 2)

            @pl.when(jnp.logical_not(safe))
            def _():
                running[...] = jnp.full_like(running, masked_score)

                def add(j, s):
                    old = running[...]
                    new = jnp.maximum(old, jnp.max(s, axis=0, keepdims=True))
                    e = jnp.exp2(s - new).astype(jnp.bfloat16)
                    weighted[...] = weighted[...] * jnp.exp2(old - new) + jnp.dot(
                        values(j), e, preferred_element_type=jnp.float32
                    )
                    running[...] = new

                def one(j, carry):
                    add(j, scores(j))
                    return carry

                lax.fori_loop(0, full, one, 0)

                @pl.when(left > 0)
                def _():
                    s = scores(full)
                    add(full, jnp.where(inside(s.shape), s, masked_score))

            maps = weighted[0:HEAD, :] / weighted[HEAD : HEAD + 1, :]
            mix = maps[:, 0:size] - lam_ref[here // parts] * maps[:, size:pair]
            normed = mix * lax.rsqrt(jnp.mean(mix * mix, axis=0, keepdims=True) + epsilon)
            normed = normed * gain
            position = first + lax.broadcasted_iota(jnp.int32, (1, size), 1)
            out_ref[tile] = jnp.where(position < live, normed, 0.0).astype(jnp.bfloat16)

        return carry

    lax.fori_loop(0, chunks * heads, tile_body, 0)
    for c in range(chunks):
        for d in range(heads):
            out_refs[d][c] = out_ref[c * heads + d]


def diff_part(scal, mix_lambda, gain, kvs, qs, chunks, rows, parts):
    heads = len(qs) // chunks
    count = heads * parts
    size = rows // chunks
    blocks = (*kvs, *qs)
    return pl.pallas_call(
        functools.partial(diff_kernel, chunks, rows, parts, count),
        in_specs=[smem(), smem(), whole(gain.shape)] + [whole(a.shape) for a in blocks],
        out_specs=[whole((chunks, HEAD, size))] * heads,
        out_shape=[jax.ShapeDtypeStruct((chunks, HEAD, size), jnp.bfloat16)] * heads,
        scratch_shapes=[
            pltpu.VMEM((chunks * heads, HEAD, size), jnp.bfloat16),
            pltpu.VMEM((rows * count, 2 * HEAD), jnp.bfloat16),
            pltpu.VMEM((HEAD + 16, rows * count), jnp.bfloat16),
            pltpu.VMEM((chunks * heads, 2 * HEAD, 2 * size), jnp.bfloat16),
            pltpu.VMEM((HEAD + 16, 2 * size), jnp.float32),
            pltpu.VMEM((1, 2 * size), jnp.float32),
        ],
        grid=(1,),
        compiler_params=pltpu.CompilerParams(vmem_limit_bytes=32 << 20),
        cost_estimate=cost(1000 * heads * rows * rows * count),
        name="differential",
    )(scal, mix_lambda, gain, *blocks)


def out_kernel(heads, parts, begin, scal_ref, win_keep_ref, win_send_ref, *refs):
    diff_refs = refs[:heads]
    win_w_ref, diff_w_ref, keep_ref, send_ref, stacked = refs[heads:]
    here, core = scal_ref[0] // parts, scal_ref[2] % 2
    half = stacked.shape[1]
    win_width = win_keep_ref.shape[1]

    @pl.when(pl.program_id(0) == 0)
    def _():
        stacked[0, :, 0:win_width] = win_keep_ref[...]
        stacked[1, :, 0:win_width] = win_send_ref[...]
        pieces = []
        for h in range(heads):
            piece = diff_refs[0][0]
            for d in range(1, heads):
                piece = jnp.where((here ^ d) == h, diff_refs[d][0], piece)
            pieces.append(piece)
        turned = jnp.transpose(jnp.concatenate(pieces, axis=0).astype(jnp.float32))
        turned = turned.astype(jnp.bfloat16)
        stacked[core, :, win_width:] = turned[0:half]
        stacked[1 - core, :, win_width:] = turned[half:]

    block = keep_ref.shape[1]
    at = pl.multiple_of(begin + pl.program_id(0) * block, block)
    lanes = pl.ds(at, block)
    weight = jnp.concatenate([win_w_ref[:, lanes], diff_w_ref[:, lanes]], axis=0)
    for i, ref in enumerate((keep_ref, send_ref)):
        ref[...] = jnp.dot(stacked[i], weight, preferred_element_type=jnp.float32).astype(
            jnp.bfloat16
        )


def out_part(scal, offset, win_rows, diffs, win_out, diff_out, begin, width, block, parts):
    heads = len(diffs)
    depth = win_out.shape[0] + diff_out.shape[0]
    size = diffs[0].shape[2]
    half = size // 2
    q_width = win_rows.shape[1]

    def rows_at(bit):
        return lambda j, scal: (scal[2] ^ (2 * offset + bit), 0)

    grid_spec = pltpu.PrefetchScalarGridSpec(
        num_scalar_prefetch=1,
        grid=(width // block,),
        in_specs=[pl.BlockSpec((half, q_width), rows_at(bit)) for bit in range(2)]
        + [
            pl.BlockSpec((1, HEAD, size), lambda j, scal: ((scal[2] // 2) ^ offset, 0, 0))
            for _ in diffs
        ]
        + [pl.BlockSpec(memory_space=pltpu.VMEM)] * 2,
        out_specs=[pl.BlockSpec((half, block), lambda j, scal: (0, j))] * 2,
        scratch_shapes=[pltpu.VMEM((2, half, depth), jnp.bfloat16)],
    )
    return pl.pallas_call(
        functools.partial(out_kernel, heads, parts, begin),
        grid_spec=grid_spec,
        out_shape=[jax.ShapeDtypeStruct((half, width), jnp.bfloat16)] * 2,
        compiler_params=pltpu.CompilerParams(
            dimension_semantics=("arbitrary",), vmem_limit_bytes=16 << 20
        ),
        cost_estimate=cost(2 * size * depth * width),
        name="project_out",
    )(scal, win_rows, win_rows, *diffs, win_out, diff_out)


def body(
    inputs,
    length,
    win_query,
    win_key,
    win_value,
    sink_logit,
    diff_query,
    diff_key,
    diff_value,
    mix_lambda,
    head_gain,
    win_out,
    diff_out,
):
    rows = inputs.shape[0]
    sp, tp = lax.axis_size("sp"), lax.axis_size("tp")
    chips = tp // 2
    size = rows // chips
    heads = mix_lambda.shape[0]
    parts = sp // heads
    here, me = lax.axis_index("sp"), lax.axis_index("tp")
    weights = (win_query, win_key, win_value, diff_query, diff_key, diff_value)
    steps = 2
    scal = jnp.stack([here, length[0], me]).astype(jnp.int32)
    far_weights = fetch(scal, weights, list(range(2, tp)), tp)
    out_weights = fetch(scal, (win_out, diff_out), [None], tp)

    pieces = [inputs[c * size : (c + 1) * size] for c in range(chips)]
    far = [
        [lax.ppermute(pieces[c], "tp", flip("tp", 2 * o)) for o in range(1, chips)]
        for c in range(chips)
    ]
    sib = lax.ppermute(inputs, "tp", flip("tp", 1))
    acc = project_near(inputs, sib, weights, scal, steps)
    q_parts, kv_parts, kvs, qs = [], [], [], []
    for c in range(chips):
        xs = []
        for piece in far[c]:
            xs += [piece, lax.ppermute(piece, "tp", flip("tp", 1))]
        q_t, kv, *slots = project_far(acc, c, size, xs, far_weights, scal, heads, parts)
        q_parts.append(q_t)
        kv_parts.append(kv)
        moved = [slots[0]]
        for d in range(1, heads):
            moved.append(lax.ppermute(slots[d], "sp", flip("sp", d * parts)))
        mine = jnp.stack([m[:size] for m in moved])
        kvs += [mine] + [lax.ppermute(mine, "sp", flip("sp", e)) for e in range(1, parts)]
        qs += moved

    up = [(i, i + 1) for i in range(sp - 1)]
    down = [(i + 1, i) for i in range(sp - 1)]
    low = lax.ppermute(kv_parts[-1][size - WINDOW :], "sp", up)
    high = lax.ppermute(kv_parts[0][:WINDOW], "sp", down)
    win_rows = window_part(scal, sink_logit, q_parts, kv_parts, low, high)

    gain = head_gain.reshape(1, HEAD)
    mixed = diff_part(scal, mix_lambda, gain, kvs, qs, chips, rows, parts)
    diffs = [mixed[0]]
    for d in range(1, heads):
        diffs.append(lax.ppermute(mixed[d], "sp", flip("sp", d * parts)))

    width = win_out.shape[1]
    block = width // 4

    def project(o, begin, end):
        return out_part(
            scal, o, win_rows, diffs, *out_weights, begin, end - begin, block, parts
        )

    def add(*values):
        return functools.reduce(lambda a, b: a + b, [v.astype(jnp.float32) for v in values])

    cuts = (0, width // 4, width)
    arrived = []
    for begin, end in zip(cuts[:-1], cuts[1:]):
        count = 1 if begin == 0 else 2
        span = (end - begin) // count
        crossed = [[] for _ in range(count)]
        for o in range(1, chips):
            keep, away = project(o, begin, end)
            other = lax.ppermute(away, "tp", flip("tp", 1))
            pair = add(keep, other).astype(jnp.bfloat16)
            for i in range(count):
                piece = pair[:, i * span : (i + 1) * span]
                crossed[i].append(lax.ppermute(piece, "tp", flip("tp", 2 * o)))
        arrived += crossed
    keep, away = project(0, 0, width)
    other = lax.ppermute(away, "tp", flip("tp", 1))
    outs, begin = [], 0
    for crossed in arrived:
        end = begin + crossed[0].shape[1]
        outs.append(add(keep[:, begin:end], other[:, begin:end], *crossed).astype(jnp.bfloat16))
        begin = end
    return jnp.concatenate(outs, axis=1)


def solution(mesh):
    placed = (
        P("sp", "tp"),
        P(),
        P(None, "tp"),
        P(None, "tp"),
        P(None, "tp"),
        P("tp"),
        P(None, "tp"),
        P(None, "tp"),
        P(None, "tp"),
        P("tp"),
        P(),
        P("tp", None),
        P("tp", None),
    )

    return jax.shard_map(
        body, mesh=mesh, in_specs=placed, out_specs=P(("sp", "tp"), None), check_vma=False
    )
```

```python
import functools
import math

import jax
import jax.numpy as jnp
from jax import lax
from jax.experimental import pallas as pl
from jax.experimental.pallas import tpu as pltpu
from jax.sharding import PartitionSpec as P

HEAD = 64
DQK = 32
GROUP = 3
WINDOW = 128

epsilon = 1e-06
masked_score = -1e30
LOG2E = math.log2(math.e)
SAFE_BOUND = 90.0


def vmem():
    return pl.BlockSpec(memory_space=pltpu.VMEM)


def smem():
    return pl.BlockSpec(memory_space=pltpu.SMEM)


def cost(flops, bytes_accessed=0, transcendentals=0):
    return pl.CostEstimate(
        flops=flops, bytes_accessed=bytes_accessed, transcendentals=transcendentals
    )


def flip(axis, bits):
    return [(i, i ^ bits) for i in range(lax.axis_size(axis))]


def near_kernel(scal_ref, own_ref, sib_ref, *refs):
    weight_refs, acc_ref = refs[:-1], refs[-1]
    depth = own_ref.shape[1]
    me = scal_ref[2]
    low = 0
    for group in ((0, 1), (2, 3), (4,), (5,)):
        total = None
        for x_ref, k in ((own_ref, 0), (sib_ref, 1)):
            at = pl.multiple_of((me ^ k) * depth, depth)
            weight = jnp.concatenate([weight_refs[i][pl.ds(at, depth), :] for i in group], axis=1)
            added = jnp.dot(x_ref[...], weight, preferred_element_type=jnp.float32)
            total = added if total is None else total + added
        acc_ref[:, low : low + total.shape[1]] = total
        low += total.shape[1]


def project_near(own, sib, weights, scal):
    rows, depth = own.shape
    width = sum(w.shape[1] for w in weights)
    return pl.pallas_call(
        near_kernel,
        in_specs=[smem()] + [vmem()] * 8,
        out_specs=vmem(),
        out_shape=jax.ShapeDtypeStruct((rows, width), jnp.float32),
        compiler_params=pltpu.CompilerParams(vmem_limit_bytes=24 << 20),
        cost_estimate=cost(4 * rows * depth * width),
        name="project_near",
    )(scal, own, sib, *weights)


def copy_kernel(begin, *refs):
    count = len(refs) // 2
    sources, targets, semaphores = refs[:count], refs[count : 2 * count], refs[2 * count]
    copies = [
        pltpu.make_async_copy(
            source.at[pl.ds(begin, target.shape[0]), :], target, semaphores.at[i]
        )
        for i, (source, target) in enumerate(zip(sources, targets))
    ]
    for copy in copies:
        copy.start()
    for copy in copies:
        copy.wait()


def fetch(arrays, begin=0, rows=None, room=1 << 20):
    shapes = [(a.shape[0] if rows is None else rows, a.shape[1]) for a in arrays]
    return pl.pallas_call(
        functools.partial(copy_kernel, begin),
        in_specs=[pl.BlockSpec(memory_space=pltpu.HBM)] * len(arrays),
        out_specs=[pl.BlockSpec(memory_space=pltpu.VMEM)] * len(arrays),
        out_shape=[pltpu.VMEM(shape, jnp.bfloat16) for shape in shapes],
        scratch_shapes=[pltpu.SemaphoreType.DMA((len(arrays),))],
        compiler_params=pltpu.CompilerParams(vmem_limit_bytes=room),
        cost_estimate=cost(1 << 30),
        name="fetch",
    )(*arrays)


def far_kernel(begin, count, heads, parts, scal_ref, acc_ref, *refs):
    xs = refs[:count]
    weight_refs = refs[count : count + 6]
    qt_ref, kv_ref = refs[count + 6 : count + 8]
    slot_refs = refs[count + 8 : count + 8 + heads]
    buf_ref = refs[count + 8 + heads]
    rows, depth = xs[0].shape
    here = scal_ref[0] // parts

    def project(which):
        low = sum(weight_refs[i].shape[1] for i in range(which[0]))
        span = sum(weight_refs[i].shape[1] for i in which)
        total = acc_ref[begin : begin + rows, low : low + span]
        for n, x in enumerate(xs):
            at = pl.multiple_of((scal_ref[2] ^ (2 + n)) * depth, depth)
            weight = jnp.concatenate([weight_refs[i][pl.ds(at, depth), :] for i in which], axis=1)
            total += jnp.dot(x[...], weight, preferred_element_type=jnp.float32)
        ends = [sum(weight_refs[i].shape[1] for i in which[:n]) for n in range(len(which) + 1)]
        return [total[:, a:b] for a, b in zip(ends[:-1], ends[1:])]

    diff_k, diff_v = project((4, 5))
    win_v, diff_q = project((2, 3))
    win_q, win_k = project((0, 1))
    diff_q = diff_q * (LOG2E * DQK ** (-0.5))
    for h in range(heads):
        lanes = slice(h * HEAD, (h + 1) * HEAD)
        q, k, v = diff_q[:, lanes], diff_k[:, lanes], diff_v[:, lanes]
        buf_ref[h, 0:rows, :] = jnp.concatenate([k, v], axis=1).astype(jnp.bfloat16)
        pair = jnp.concatenate([q[: rows // 2], q[rows // 2 :]], axis=1)
        buf_ref[h, rows : rows + rows // 2, :] = pair.astype(jnp.bfloat16)
    for slot in range(heads):
        slot_refs[slot][...] = buf_ref[slot ^ here]
    qt_ref[...] = jnp.transpose(win_q * (LOG2E * HEAD ** (-0.5))).astype(jnp.bfloat16)
    kv_ref[...] = jnp.concatenate([win_k, win_v], axis=1).astype(jnp.bfloat16)


def project_far(acc, chunk, rows, xs, weights, scal, heads, parts):
    depth = xs[0].shape[1]
    count = len(xs)
    width = acc.shape[1]
    kv_width = weights[1].shape[1] + weights[2].shape[1]
    q_width = weights[0].shape[1]
    shapes = [(q_width, rows), (rows, kv_width)] + [(rows + rows // 2, 2 * HEAD)] * heads
    return pl.pallas_call(
        functools.partial(far_kernel, chunk * rows, count, heads, parts),
        in_specs=[smem()] + [vmem()] * (1 + count + 6),
        out_specs=[vmem() for shape in shapes],
        out_shape=[jax.ShapeDtypeStruct(shape, jnp.bfloat16) for shape in shapes],
        scratch_shapes=[pltpu.VMEM((heads, rows + rows // 2, 2 * HEAD), jnp.bfloat16)],
        compiler_params=pltpu.CompilerParams(vmem_limit_bytes=24 << 20),
        cost_estimate=cost(2 * count * rows * depth * width),
        name="project_far",
    )(scal, acc, *xs, *weights)


def window_kernel(begin, whole_rows, kv_local, scal_ref, sink_ref, *refs):
    q_ref, low_ref, kv_ref, high_ref, rows_ref, keys, values_t, out_ref = refs
    last = low_ref.shape[0] - WINDOW
    here, live = scal_ref[0], scal_ref[1]
    rows = kv_ref.shape[0]
    span = rows + 2 * WINDOW
    keys[0:WINDOW, :] = low_ref[last:, :]
    keys[WINDOW : WINDOW + rows, :] = kv_ref[...]
    keys[WINDOW + rows : span, :] = high_ref[0:WINDOW, :]
    k_width = kv_local * HEAD
    turned = jnp.transpose(keys[:, k_width:].astype(jnp.float32)).astype(jnp.bfloat16)
    tail = (lax.broadcasted_iota(jnp.int32, (16, span), 0) == 0).astype(jnp.bfloat16)
    for h in range(kv_local):
        values_t[h, 0:HEAD, :] = turned[h * HEAD : (h + 1) * HEAD]
        values_t[h, HEAD : HEAD + 16, :] = tail
    step = 128
    for b in range(rows // step):
        first = here * whole_rows + begin + b * step

        @pl.when(first >= live)
        def _():
            out_ref[:, b * step : (b + 1) * step] = jnp.zeros(
                (out_ref.shape[0], step), jnp.float32
            )

        @pl.when(first < live)
        def _():
            wide = step + 2 * WINDOW
            at = b * step
            key_at = lax.broadcasted_iota(jnp.int32, (wide, step), 0)
            query_at = lax.broadcasted_iota(jnp.int32, (wide, step), 1)
            key_pos = first - WINDOW + key_at
            gap = key_at - WINDOW - query_at
            allowed = (
                (gap <= WINDOW) & (gap >= -WINDOW) & (key_pos >= 0) & (key_pos < live)
            )
            live_row = (
                first + lax.broadcasted_iota(jnp.int32, (1, step), 1)
            ) < live
            for h in range(kv_local):
                key_block = keys[b * step : b * step + wide, h * HEAD : (h + 1) * HEAD]
                value_block = values_t[h, :, b * step : b * step + wide]
                for g in range(GROUP):
                    head = h * GROUP + g
                    q = q_ref[head * HEAD : (head + 1) * HEAD, at : at + step]
                    s = jnp.dot(key_block, q, preferred_element_type=jnp.float32)
                    s = jnp.where(allowed, s, masked_score)
                    sink = sink_ref[head] * LOG2E
                    top = jnp.maximum(jnp.max(s, axis=0, keepdims=True), sink)
                    e = jnp.exp2(s - top).astype(jnp.bfloat16)
                    mixed = jnp.dot(value_block, e, preferred_element_type=jnp.float32)
                    total = mixed[HEAD : HEAD + 1] + jnp.exp2(sink - top)
                    result = jnp.where(live_row, mixed[0:HEAD] / total, 0.0)
                    out_ref[head * HEAD : (head + 1) * HEAD, b * step : (b + 1) * step] = (
                        result
                    )

        block = out_ref[:, b * step : (b + 1) * step]
        rows_ref[b * step : (b + 1) * step, :] = jnp.transpose(block).astype(jnp.bfloat16)


def window_part(scal, sink_logit, q_t, low, kv, high, begin, whole_rows):
    q_width, rows = q_t.shape
    kv_width = kv.shape[1]
    kv_local = kv_width // (2 * HEAD)
    return pl.pallas_call(
        functools.partial(window_kernel, begin, whole_rows, kv_local),
        in_specs=[smem()] * 2 + [vmem()] * 4,
        out_specs=vmem(),
        out_shape=jax.ShapeDtypeStruct((rows, q_width), jnp.bfloat16),
        scratch_shapes=[
            pltpu.VMEM((rows + 2 * WINDOW, kv_width), jnp.bfloat16),
            pltpu.VMEM((kv_local, HEAD + 16, rows + 2 * WINDOW), jnp.bfloat16),
            pltpu.VMEM((q_width, rows), jnp.float32),
        ],
        compiler_params=pltpu.CompilerParams(vmem_limit_bytes=16 << 20),
        cost_estimate=cost(40 * q_width * rows * 384),
        name="window",
    )(scal, sink_logit, q_t, low, kv, high)


def diff_kernel(chunks, rows, parts, count, scal_ref, lam_ref, gain_ref, *refs):
    heads = count // parts
    kv_refs = refs[: chunks * parts]
    q_refs = refs[chunks * parts : chunks * (parts + heads)]
    out_refs = refs[chunks * (parts + heads) : chunks * (parts + heads) + heads]
    out_ref, keys, values_t, queries, weighted, running = refs[-6:]
    here, live = scal_ref[0], scal_ref[1]
    size = rows // chunks
    total = rows * count
    step = 512
    pair = 2 * size

    top_key = jnp.zeros((1, 2 * HEAD), jnp.float32)
    queries[...] = jnp.zeros_like(queries)
    for c in range(chunks):
        for d in range(count):
            at = pl.multiple_of((here ^ d) * rows + c * size, size)
            block = kv_refs[c * parts + d % parts][d // parts]
            keys[pl.ds(at, size), :] = block
            wide = block.astype(jnp.float32)
            top_key = jnp.maximum(top_key, jnp.max(jnp.abs(wide), axis=0, keepdims=True))
            alive = (at + lax.broadcasted_iota(jnp.int32, (1, size), 1)) < live
            turned = jnp.where(alive, jnp.transpose(wide)[HEAD:], 0.0)
            values_t[0:HEAD, pl.ds(at, size)] = turned.astype(jnp.bfloat16)
            if d % parts == 0:
                half = size // 2
                pairs = q_refs[c * heads + d // parts][size : size + half, :]
                turned = jnp.transpose(pairs.astype(jnp.float32))
                turned = jnp.concatenate([turned[0:HEAD], turned[HEAD:]], axis=1)
                turned = turned.astype(jnp.bfloat16)
                tile = c * heads + d // parts
                queries[tile, 0:DQK, 0:size] = turned[0:DQK]
                queries[tile, DQK : 2 * DQK, size:pair] = turned[DQK:]
    counted = lax.broadcasted_iota(jnp.int32, (16, total), 0) == 0
    counted &= lax.broadcasted_iota(jnp.int32, (16, total), 1) < live
    values_t[HEAD : HEAD + 16, :] = counted.astype(jnp.bfloat16)
    limit = jnp.transpose(jnp.broadcast_to(top_key, (8, 2 * HEAD)))[:, 0:1]
    gain = jnp.transpose(jnp.broadcast_to(gain_ref[...], (8, HEAD)))[:, 0:1]

    full = live // step
    left = live - full * step

    def tile_body(tile, carry):
        c, zd = tile // heads, tile % heads
        first = (here ^ (zd * parts)) * rows + c * size

        @pl.when(first >= live)
        def _():
            out_ref[tile] = jnp.zeros(out_ref.shape[1:], out_ref.dtype)

        @pl.when(first < live)
        def _():
            q = queries[tile]
            bound = jnp.max(jnp.sum(jnp.abs(q.astype(jnp.float32)) * limit, axis=0, keepdims=True))
            safe = bound < SAFE_BOUND

            def scores(j):
                at = pl.multiple_of(j * step, step)
                return jnp.dot(keys[pl.ds(at, step), :], q, preferred_element_type=jnp.float32)

            def values(j):
                return values_t[:, pl.ds(pl.multiple_of(j * step, step), step)]

            def inside(shape):
                return lax.broadcasted_iota(jnp.int32, shape, 0) < left

            weighted[...] = jnp.zeros_like(weighted)

            @pl.when(safe)
            def _():
                def several(j, number):
                    raised = [jnp.exp2(scores(j + i)).astype(jnp.bfloat16) for i in range(number)]
                    added = [
                        jnp.dot(values(j + i), e, preferred_element_type=jnp.float32)
                        for i, e in enumerate(raised)
                    ]
                    weighted[...] += functools.reduce(lambda a, b: a + b, added)

                def one(j, carry):
                    several(4 * j, 4)
                    return carry

                pairs = (live + 2 * step - 1) // (2 * step)
                lax.fori_loop(0, pairs // 2, one, 0)

                @pl.when(pairs % 2 == 1)
                def _():
                    several(2 * (pairs - 1), 2)

            @pl.when(jnp.logical_not(safe))
            def _():
                running[...] = jnp.full_like(running, masked_score)

                def add(j, s):
                    old = running[...]
                    new = jnp.maximum(old, jnp.max(s, axis=0, keepdims=True))
                    e = jnp.exp2(s - new).astype(jnp.bfloat16)
                    weighted[...] = weighted[...] * jnp.exp2(old - new) + jnp.dot(
                        values(j), e, preferred_element_type=jnp.float32
                    )
                    running[...] = new

                def one(j, carry):
                    add(j, scores(j))
                    return carry

                lax.fori_loop(0, full, one, 0)

                @pl.when(left > 0)
                def _():
                    s = scores(full)
                    add(full, jnp.where(inside(s.shape), s, masked_score))

            maps = weighted[0:HEAD, :] / weighted[HEAD : HEAD + 1, :]
            mix = maps[:, 0:size] - lam_ref[here // parts] * maps[:, size:pair]
            normed = mix * lax.rsqrt(jnp.mean(mix * mix, axis=0, keepdims=True) + epsilon)
            normed = normed * gain
            position = first + lax.broadcasted_iota(jnp.int32, (1, size), 1)
            out_ref[tile] = jnp.where(position < live, normed, 0.0).astype(jnp.bfloat16)

        return carry

    lax.fori_loop(0, chunks * heads, tile_body, 0)
    for c in range(chunks):
        for d in range(heads):
            out_refs[d][c] = out_ref[c * heads + d]


def diff_part(scal, mix_lambda, gain, kvs, qs, chunks, rows, parts):
    heads = len(qs) // chunks
    count = heads * parts
    size = rows // chunks
    blocks = (*kvs, *qs)
    return pl.pallas_call(
        functools.partial(diff_kernel, chunks, rows, parts, count),
        in_specs=[smem()] * 2 + [vmem()] * (1 + len(blocks)),
        out_specs=[vmem()] * heads,
        out_shape=[jax.ShapeDtypeStruct((chunks, HEAD, size), jnp.bfloat16)] * heads,
        scratch_shapes=[
            pltpu.VMEM((chunks * heads, HEAD, size), jnp.bfloat16),
            pltpu.VMEM((rows * count, 2 * HEAD), jnp.bfloat16),
            pltpu.VMEM((HEAD + 16, rows * count), jnp.bfloat16),
            pltpu.VMEM((chunks * heads, 2 * HEAD, 2 * size), jnp.bfloat16),
            pltpu.VMEM((HEAD + 16, 2 * size), jnp.float32),
            pltpu.VMEM((1, 2 * size), jnp.float32),
        ],
        compiler_params=pltpu.CompilerParams(vmem_limit_bytes=32 << 20),
        cost_estimate=cost(1000 * heads * rows * rows * count),
        name="differential",
    )(scal, mix_lambda, gain, *blocks)


def out_kernel(heads, parts, offset, begin, scal_ref, win_ref, *refs):
    diff_refs = refs[:heads]
    win_w_ref, diff_w_ref, keep_ref, send_ref, stacked = refs[heads:]
    here, me = scal_ref[0] // parts, scal_ref[2]
    chip, core = (me // 2) ^ offset, me % 2
    half = stacked.shape[1]
    win_width = win_ref.shape[1]

    @pl.when(pl.program_id(0) == 0)
    def _():
        for bit in range(2):
            at = pl.multiple_of((me ^ (2 * offset + bit)) * half, half)
            stacked[bit, :, 0:win_width] = win_ref[pl.ds(at, half), :]
        pieces = []
        for h in range(heads):
            piece = diff_refs[0][chip]
            for d in range(1, heads):
                piece = jnp.where((here ^ d) == h, diff_refs[d][chip], piece)
            pieces.append(piece)
        turned = jnp.transpose(jnp.concatenate(pieces, axis=0).astype(jnp.float32))
        turned = turned.astype(jnp.bfloat16)
        stacked[core, :, win_width:] = turned[0:half]
        stacked[1 - core, :, win_width:] = turned[half:]

    block = keep_ref.shape[1]
    at = pl.multiple_of(begin + pl.program_id(0) * block, block)
    lanes = pl.ds(at, block)
    weight = jnp.concatenate([win_w_ref[:, lanes], diff_w_ref[:, lanes]], axis=0)
    for i, ref in enumerate((keep_ref, send_ref)):
        ref[...] = jnp.dot(stacked[i], weight, preferred_element_type=jnp.float32).astype(
            jnp.bfloat16
        )


def out_part(scal, offset, win_rows, diffs, win_out, diff_out, begin, width, block, parts):
    heads = len(diffs)
    depth = win_out.shape[0] + diff_out.shape[0]
    size = diffs[0].shape[2]
    half = size // 2

    return pl.pallas_call(
        functools.partial(out_kernel, heads, parts, offset, begin),
        in_specs=[smem()] + [vmem()] * (3 + heads),
        out_specs=[pl.BlockSpec((half, block), lambda j: (0, j))] * 2,
        scratch_shapes=[pltpu.VMEM((2, half, depth), jnp.bfloat16)],
        grid=(width // block,),
        out_shape=[jax.ShapeDtypeStruct((half, width), jnp.bfloat16)] * 2,
        compiler_params=pltpu.CompilerParams(
            dimension_semantics=("arbitrary",), vmem_limit_bytes=16 << 20
        ),
        cost_estimate=cost(2 * size * depth * width),
        name="project_out",
    )(scal, win_rows, *diffs, win_out, diff_out)


def body(
    inputs,
    length,
    win_query,
    win_key,
    win_value,
    sink_logit,
    diff_query,
    diff_key,
    diff_value,
    mix_lambda,
    head_gain,
    win_out,
    diff_out,
):
    rows = inputs.shape[0]
    sp, tp = lax.axis_size("sp"), lax.axis_size("tp")
    chips = tp // 2
    size = rows // chips
    heads = mix_lambda.shape[0]
    parts = sp // heads
    here, me = lax.axis_index("sp"), lax.axis_index("tp")
    weights = (win_query, win_key, win_value, diff_query, diff_key, diff_value)
    scal = jnp.stack([here, length[0], me]).astype(jnp.int32)
    weights = fetch(weights, room=46 << 20)
    out_weights = fetch((win_out, diff_out), room=38 << 20)

    pieces = []
    for c in range(chips):
        pieces += fetch((inputs,), c * size, size)
    far = [
        [lax.ppermute(pieces[c], "tp", flip("tp", 2 * o)) for o in range(1, chips)]
        for c in range(chips)
    ]
    sib = lax.ppermute(inputs, "tp", flip("tp", 1))
    acc = project_near(inputs, sib, weights, scal)
    q_parts, kv_parts, kvs, qs = [], [], [], []
    for c in range(chips):
        xs = []
        for piece in far[c]:
            xs += [piece, lax.ppermute(piece, "tp", flip("tp", 1))]
        q_t, kv, *slots = project_far(acc, c, size, xs, weights, scal, heads, parts)
        q_parts.append(q_t)
        kv_parts.append(kv)
        moved = [slots[0]]
        for d in range(1, heads):
            moved.append(lax.ppermute(slots[d], "sp", flip("sp", d * parts)))
        mine = jnp.stack([m[:size] for m in moved])
        kvs += [mine] + [lax.ppermute(mine, "sp", flip("sp", e)) for e in range(1, parts)]
        qs += moved

    up = [(i, i + 1) for i in range(sp - 1)]
    down = [(i + 1, i) for i in range(sp - 1)]
    low = lax.ppermute(kv_parts[-1][size - WINDOW :], "sp", up)
    high = lax.ppermute(kv_parts[0][:WINDOW], "sp", down)
    edges = [low, *kv_parts, high]
    win_rows = []
    for c in range(chips):
        win_rows.append(
            window_part(scal, sink_logit, q_parts[c], *edges[c : c + 3], c * size, rows)
        )
    win_rows = jnp.concatenate(win_rows)

    gain = head_gain.reshape(1, HEAD)
    mixed = diff_part(scal, mix_lambda, gain, kvs, qs, chips, rows, parts)
    diffs = [mixed[0]]
    for d in range(1, heads):
        diffs.append(lax.ppermute(mixed[d], "sp", flip("sp", d * parts)))

    width = win_out.shape[1]
    block = width // 4

    def project(o, begin, end):
        return out_part(
            scal, o, win_rows, diffs, *out_weights, begin, end - begin, block, parts
        )

    def add(*values):
        return functools.reduce(lambda a, b: a + b, [v.astype(jnp.float32) for v in values])

    cuts = (0, width // 4, width // 2, width)
    arrived = []
    for begin, end in zip(cuts[:-1], cuts[1:]):
        count = (end - begin) // block
        span = (end - begin) // count
        crossed = [[] for _ in range(count)]
        for o in range(1, chips):
            keep, away = project(o, begin, end)
            other = lax.ppermute(away, "tp", flip("tp", 1))
            pair = add(keep, other).astype(jnp.bfloat16)
            for i in range(count):
                piece = pair[:, i * span : (i + 1) * span]
                crossed[i].append(lax.ppermute(piece, "tp", flip("tp", 2 * o)))
        arrived += crossed
    keep, away = project(0, 0, width)
    other = lax.ppermute(away, "tp", flip("tp", 1))
    outs, begin = [], 0
    for crossed in arrived:
        end = begin + crossed[0].shape[1]
        outs.append(add(keep[:, begin:end], other[:, begin:end], *crossed).astype(jnp.bfloat16))
        begin = end
    return jnp.concatenate(outs, axis=1)


def solution(mesh):
    placed = (
        P("sp", "tp"),
        P(),
        P(None, "tp"),
        P(None, "tp"),
        P(None, "tp"),
        P("tp"),
        P(None, "tp"),
        P(None, "tp"),
        P(None, "tp"),
        P("tp"),
        P(),
        P("tp", None),
        P("tp", None),
    )

    return jax.shard_map(
        body, mesh=mesh, in_specs=placed, out_specs=P(("sp", "tp"), None), check_vma=False
    )
```

```python
import functools
import math

import jax
import jax.numpy as jnp
from jax import lax
from jax.experimental import pallas as pl
from jax.experimental.pallas import tpu as pltpu
from jax.sharding import PartitionSpec as P

HEAD = 64
DQK = 32
GROUP = 3
WINDOW = 128

epsilon = 1e-06
masked_score = -1e30
LOG2E = math.log2(math.e)
SAFE_BOUND = 90.0


def vmem():
    return pl.BlockSpec(memory_space=pltpu.VMEM)


def smem():
    return pl.BlockSpec(memory_space=pltpu.SMEM)


def cost(flops, bytes_accessed=0, transcendentals=0):
    return pl.CostEstimate(
        flops=flops, bytes_accessed=bytes_accessed, transcendentals=transcendentals
    )


def flip(axis, bits):
    return [(i, i ^ bits) for i in range(lax.axis_size(axis))]


def near_kernel(scal_ref, own_ref, sib_ref, *refs):
    weight_refs, acc_ref = refs[:-1], refs[-1]
    depth = own_ref.shape[1]
    me = scal_ref[2]
    low = 0
    for group in ((0, 1), (2, 3), (4,), (5,)):
        total = None
        for x_ref, k in ((own_ref, 0), (sib_ref, 1)):
            at = pl.multiple_of((me ^ k) * depth, depth)
            weight = jnp.concatenate([weight_refs[i][pl.ds(at, depth), :] for i in group], axis=1)
            added = jnp.dot(x_ref[...], weight, preferred_element_type=jnp.float32)
            total = added if total is None else total + added
        acc_ref[:, low : low + total.shape[1]] = total
        low += total.shape[1]


def project_near(own, sib, weights, scal):
    rows, depth = own.shape
    width = sum(w.shape[1] for w in weights)
    return pl.pallas_call(
        near_kernel,
        in_specs=[smem()] + [vmem()] * 8,
        out_specs=vmem(),
        out_shape=jax.ShapeDtypeStruct((rows, width), jnp.float32),
        compiler_params=pltpu.CompilerParams(vmem_limit_bytes=24 << 20),
        cost_estimate=cost(4 * rows * depth * width),
    )(scal, own, sib, *weights)


def copy_kernel(begin, *refs):
    count = len(refs) // 2
    sources, targets, semaphores = refs[:count], refs[count : 2 * count], refs[2 * count]
    copies = [
        pltpu.make_async_copy(
            source.at[pl.ds(begin, target.shape[0]), :], target, semaphores.at[i]
        )
        for i, (source, target) in enumerate(zip(sources, targets))
    ]
    for copy in copies:
        copy.start()
    for copy in copies:
        copy.wait()


def fetch(arrays, begin=0, rows=None, room=1 << 20):
    shapes = [(a.shape[0] if rows is None else rows, a.shape[1]) for a in arrays]
    return pl.pallas_call(
        functools.partial(copy_kernel, begin),
        in_specs=[pl.BlockSpec(memory_space=pltpu.HBM)] * len(arrays),
        out_specs=[pl.BlockSpec(memory_space=pltpu.VMEM)] * len(arrays),
        out_shape=[pltpu.VMEM(shape, jnp.bfloat16) for shape in shapes],
        scratch_shapes=[pltpu.SemaphoreType.DMA((len(arrays),))],
        compiler_params=pltpu.CompilerParams(vmem_limit_bytes=room),
        cost_estimate=cost(1 << 30),
    )(*arrays)


def far_kernel(begin, count, heads, parts, scal_ref, acc_ref, *refs):
    xs = refs[:count]
    weight_refs = refs[count : count + 6]
    qt_ref, kv_ref = refs[count + 6 : count + 8]
    slot_refs = refs[count + 8 : count + 8 + heads]
    buf_ref = refs[count + 8 + heads]
    rows, depth = xs[0].shape
    here = scal_ref[0] // parts

    def project(which):
        low = sum(weight_refs[i].shape[1] for i in range(which[0]))
        span = sum(weight_refs[i].shape[1] for i in which)
        total = acc_ref[begin : begin + rows, low : low + span]
        for n, x in enumerate(xs):
            at = pl.multiple_of((scal_ref[2] ^ (2 + n)) * depth, depth)
            weight = jnp.concatenate([weight_refs[i][pl.ds(at, depth), :] for i in which], axis=1)
            total += jnp.dot(x[...], weight, preferred_element_type=jnp.float32)
        ends = [sum(weight_refs[i].shape[1] for i in which[:n]) for n in range(len(which) + 1)]
        return [total[:, a:b] for a, b in zip(ends[:-1], ends[1:])]

    diff_k, diff_v = project((4, 5))
    win_v, diff_q = project((2, 3))
    win_q, win_k = project((0, 1))
    diff_q = diff_q * (LOG2E * DQK ** (-0.5))
    for h in range(heads):
        lanes = slice(h * HEAD, (h + 1) * HEAD)
        q, k, v = diff_q[:, lanes], diff_k[:, lanes], diff_v[:, lanes]
        buf_ref[h, 0:rows, :] = jnp.concatenate([k, v], axis=1).astype(jnp.bfloat16)
        pair = jnp.concatenate([q[: rows // 2], q[rows // 2 :]], axis=1)
        buf_ref[h, rows : rows + rows // 2, :] = pair.astype(jnp.bfloat16)
    for slot in range(heads):
        slot_refs[slot][...] = buf_ref[slot ^ here]
    qt_ref[...] = jnp.transpose(win_q * (LOG2E * HEAD ** (-0.5))).astype(jnp.bfloat16)
    kv_ref[...] = jnp.concatenate([win_k, win_v], axis=1).astype(jnp.bfloat16)


def project_far(acc, chunk, rows, xs, weights, scal, heads, parts):
    depth = xs[0].shape[1]
    count = len(xs)
    width = acc.shape[1]
    kv_width = weights[1].shape[1] + weights[2].shape[1]
    q_width = weights[0].shape[1]
    shapes = [(q_width, rows), (rows, kv_width)] + [(rows + rows // 2, 2 * HEAD)] * heads
    return pl.pallas_call(
        functools.partial(far_kernel, chunk * rows, count, heads, parts),
        in_specs=[smem()] + [vmem()] * (1 + count + 6),
        out_specs=[vmem() for shape in shapes],
        out_shape=[jax.ShapeDtypeStruct(shape, jnp.bfloat16) for shape in shapes],
        scratch_shapes=[pltpu.VMEM((heads, rows + rows // 2, 2 * HEAD), jnp.bfloat16)],
        compiler_params=pltpu.CompilerParams(vmem_limit_bytes=24 << 20),
        cost_estimate=cost(2 * count * rows * depth * width),
    )(scal, acc, *xs, *weights)


def window_kernel(begin, whole_rows, kv_local, scal_ref, sink_ref, *refs):
    q_ref, low_ref, kv_ref, high_ref, rows_ref, keys, values_t, out_ref = refs
    last = low_ref.shape[0] - WINDOW
    here, live = scal_ref[0], scal_ref[1]
    rows = kv_ref.shape[0]
    span = rows + 2 * WINDOW
    keys[0:WINDOW, :] = low_ref[last:, :]
    keys[WINDOW : WINDOW + rows, :] = kv_ref[...]
    keys[WINDOW + rows : span, :] = high_ref[0:WINDOW, :]
    k_width = kv_local * HEAD
    turned = jnp.transpose(keys[:, k_width:].astype(jnp.float32)).astype(jnp.bfloat16)
    tail = (lax.broadcasted_iota(jnp.int32, (16, span), 0) == 0).astype(jnp.bfloat16)
    for h in range(kv_local):
        values_t[h, 0:HEAD, :] = turned[h * HEAD : (h + 1) * HEAD]
        values_t[h, HEAD : HEAD + 16, :] = tail
    step = 128
    for b in range(rows // step):
        first = here * whole_rows + begin + b * step

        @pl.when(first >= live)
        def _():
            out_ref[:, b * step : (b + 1) * step] = jnp.zeros(
                (out_ref.shape[0], step), jnp.float32
            )

        @pl.when(first < live)
        def _():
            wide = step + 2 * WINDOW
            at = b * step
            key_at = lax.broadcasted_iota(jnp.int32, (wide, step), 0)
            query_at = lax.broadcasted_iota(jnp.int32, (wide, step), 1)
            key_pos = first - WINDOW + key_at
            gap = key_at - WINDOW - query_at
            allowed = (
                (gap <= WINDOW) & (gap >= -WINDOW) & (key_pos >= 0) & (key_pos < live)
            )
            live_row = (
                first + lax.broadcasted_iota(jnp.int32, (1, step), 1)
            ) < live
            for h in range(kv_local):
                key_block = keys[b * step : b * step + wide, h * HEAD : (h + 1) * HEAD]
                value_block = values_t[h, :, b * step : b * step + wide]
                for g in range(GROUP):
                    head = h * GROUP + g
                    q = q_ref[head * HEAD : (head + 1) * HEAD, at : at + step]
                    s = jnp.dot(key_block, q, preferred_element_type=jnp.float32)
                    s = jnp.where(allowed, s, masked_score)
                    sink = sink_ref[head] * LOG2E
                    top = jnp.maximum(jnp.max(s, axis=0, keepdims=True), sink)
                    e = jnp.exp2(s - top).astype(jnp.bfloat16)
                    mixed = jnp.dot(value_block, e, preferred_element_type=jnp.float32)
                    total = mixed[HEAD : HEAD + 1] + jnp.exp2(sink - top)
                    result = jnp.where(live_row, mixed[0:HEAD] / total, 0.0)
                    out_ref[head * HEAD : (head + 1) * HEAD, b * step : (b + 1) * step] = (
                        result
                    )

        block = out_ref[:, b * step : (b + 1) * step]
        rows_ref[b * step : (b + 1) * step, :] = jnp.transpose(block).astype(jnp.bfloat16)


def window_part(scal, sink_logit, q_t, low, kv, high, begin, whole_rows):
    q_width, rows = q_t.shape
    kv_width = kv.shape[1]
    kv_local = kv_width // (2 * HEAD)
    return pl.pallas_call(
        functools.partial(window_kernel, begin, whole_rows, kv_local),
        in_specs=[smem()] * 2 + [vmem()] * 4,
        out_specs=vmem(),
        out_shape=jax.ShapeDtypeStruct((rows, q_width), jnp.bfloat16),
        scratch_shapes=[
            pltpu.VMEM((rows + 2 * WINDOW, kv_width), jnp.bfloat16),
            pltpu.VMEM((kv_local, HEAD + 16, rows + 2 * WINDOW), jnp.bfloat16),
            pltpu.VMEM((q_width, rows), jnp.float32),
        ],
        compiler_params=pltpu.CompilerParams(vmem_limit_bytes=16 << 20),
        cost_estimate=cost(40 * q_width * rows * 384),
    )(scal, sink_logit, q_t, low, kv, high)


def diff_kernel(chunks, rows, heads, parts, others, offset, scal_ref, *refs):
    first_call = offset is None
    kv_refs = refs[: chunks * len(others)]
    refs = refs[chunks * len(others) :]
    size = rows // chunks
    here, live = scal_ref[0], scal_ref[1]
    mine, part = here // parts, here % parts
    if first_call:
        q_refs, refs = refs[: chunks * heads], refs[chunks * heads :]
        queries, weighted, running, flags, keys, values_t = refs
    else:
        queries, weighted_in, running_in, flags, lam_ref, gain_ref = refs[:6]
        out_refs = refs[6 : 6 + heads]
        weighted, running, out_ref, keys, values_t = refs[6 + heads :]
        base = ((scal_ref[2] // 2) ^ offset) * heads
    step = 512
    pair = 2 * size
    total = keys.shape[0]

    live_keys = jnp.int32(0)
    for e in others:
        for h in range(heads):
            live_keys += jnp.clip(live - (h * parts + (part ^ e)) * rows, 0, rows)

    top_key = jnp.zeros((1, 2 * HEAD), jnp.float32)
    for n, e in enumerate(others):
        for c in range(chunks):
            for d in range(heads):
                owner, source = mine ^ d, part ^ e
                place = owner * len(others)
                if not first_call:
                    place += source - (source > part).astype(jnp.int32)
                at = pl.multiple_of(place * rows + c * size, size)
                block = kv_refs[c * len(others) + n][d]
                keys[pl.ds(at, size), :] = block
                wide = block.astype(jnp.float32)
                top_key = jnp.maximum(top_key, jnp.max(jnp.abs(wide), axis=0, keepdims=True))
                alive = (at + lax.broadcasted_iota(jnp.int32, (1, size), 1)) < live_keys
                turned = jnp.where(alive, jnp.transpose(wide)[HEAD:], 0.0)
                values_t[0:HEAD, pl.ds(at, size)] = turned.astype(jnp.bfloat16)
    counted = lax.broadcasted_iota(jnp.int32, (16, total), 0) == 0
    counted &= lax.broadcasted_iota(jnp.int32, (16, total), 1) < live_keys
    values_t[HEAD : HEAD + 16, :] = counted.astype(jnp.bfloat16)
    limit = jnp.transpose(jnp.broadcast_to(top_key, (8, 2 * HEAD)))[:, 0:1]
    if first_call:
        queries[...] = jnp.zeros_like(queries)
        for c in range(chunks):
            for d in range(heads):
                pairs = q_refs[c * heads + d][size : size + size // 2, :]
                turned = jnp.transpose(pairs.astype(jnp.float32))
                turned = jnp.concatenate([turned[0:HEAD], turned[HEAD:]], axis=1)
                turned = turned.astype(jnp.bfloat16)
                tile = c * heads + d
                queries[tile, 0:DQK, 0:size] = turned[0:DQK]
                queries[tile, DQK : 2 * DQK, size:pair] = turned[DQK:]
    else:
        gain = jnp.transpose(jnp.broadcast_to(gain_ref[...], (8, HEAD)))[:, 0:1]

    units = (live_keys + step - 1) // step

    def tile_body(index, carry):
        tile = index if first_call else base + index
        c, d = tile // heads, tile % heads
        first = (here ^ (d * parts)) * rows + c * size
        slot = tile if first_call else 0

        if first_call:
            flags[tile] = jnp.int32(0)
        else:

            @pl.when(first >= live)
            def _():
                out_ref[index] = jnp.zeros(out_ref.shape[1:], out_ref.dtype)

        @pl.when(first < live)
        def _():
            q = queries[tile]
            bound = jnp.max(jnp.sum(jnp.abs(q.astype(jnp.float32)) * limit, axis=0, keepdims=True))
            safe = bound < SAFE_BOUND
            if first_call:
                flags[tile] = safe.astype(jnp.int32)
                weighted[slot] = jnp.zeros(weighted.shape[1:], jnp.float32)
                running[slot] = jnp.where(
                    safe, jnp.zeros((1, pair), jnp.float32), masked_score
                )
            else:
                safe &= flags[tile] == 1
                weighted[slot] = weighted_in[tile]
                running[slot] = running_in[tile]

            def scores(j):
                at = pl.multiple_of(j * step, step)
                return jnp.dot(keys[pl.ds(at, step), :], q, preferred_element_type=jnp.float32)

            def values(j):
                return values_t[:, pl.ds(pl.multiple_of(j * step, step), step)]

            @pl.when(safe)
            def _():
                def several(j, number):
                    raised = [jnp.exp2(scores(j + i)).astype(jnp.bfloat16) for i in range(number)]
                    added = [
                        jnp.dot(values(j + i), e, preferred_element_type=jnp.float32)
                        for i, e in enumerate(raised)
                    ]
                    weighted[slot] += functools.reduce(lambda a, b: a + b, added)

                def one(j, carry):
                    several(4 * j, 4)
                    return carry

                lax.fori_loop(0, units // 4, one, 0)
                for number in (1, 2, 3):

                    @pl.when(units % 4 == number)
                    def _():
                        several(units - number, number)

            @pl.when(jnp.logical_not(safe))
            def _():
                def one(j, carry):
                    s = scores(j)
                    inside = lax.broadcasted_iota(jnp.int32, s.shape, 0) < live_keys - j * step
                    s = jnp.where(inside, s, masked_score)
                    old = running[slot]
                    new = jnp.maximum(old, jnp.max(s, axis=0, keepdims=True))
                    e = jnp.exp2(s - new).astype(jnp.bfloat16)
                    weighted[slot] = weighted[slot] * jnp.exp2(old - new) + jnp.dot(
                        values(j), e, preferred_element_type=jnp.float32
                    )
                    running[slot] = new
                    return carry

                lax.fori_loop(0, units, one, 0)

            if not first_call:
                maps = weighted[slot, 0:HEAD, :] / weighted[slot, HEAD : HEAD + 1, :]
                mix = maps[:, 0:size] - lam_ref[mine] * maps[:, size:pair]
                normed = mix * lax.rsqrt(jnp.mean(mix * mix, axis=0, keepdims=True) + epsilon)
                normed = normed * gain
                position = first + lax.broadcasted_iota(jnp.int32, (1, size), 1)
                out_ref[index] = jnp.where(position < live, normed, 0.0).astype(jnp.bfloat16)

        return carry

    lax.fori_loop(0, chunks * heads if first_call else heads, tile_body, 0)
    if not first_call:
        for d in range(heads):
            out_refs[d][...] = out_ref[d]


def diff_first(scal, kvs, qs, rows, parts):
    chunks = len(kvs)
    heads = len(qs) // chunks
    size = rows // chunks
    tiles = chunks * heads
    keys = rows * heads
    return pl.pallas_call(
        functools.partial(diff_kernel, chunks, rows, heads, parts, [0], None),
        in_specs=[smem()] + [vmem()] * (len(kvs) + len(qs)),
        out_specs=[vmem()] * 3 + [smem()],
        out_shape=[
            pltpu.VMEM((tiles, 2 * HEAD, 2 * size), jnp.bfloat16),
            pltpu.VMEM((tiles, HEAD + 16, 2 * size), jnp.float32),
            pltpu.VMEM((tiles, 1, 2 * size), jnp.float32),
            jax.ShapeDtypeStruct((tiles,), jnp.int32),
        ],
        scratch_shapes=[
            pltpu.VMEM((keys, 2 * HEAD), jnp.bfloat16),
            pltpu.VMEM((HEAD + 16, keys), jnp.bfloat16),
        ],
        compiler_params=pltpu.CompilerParams(vmem_limit_bytes=24 << 20),
        cost_estimate=cost(500 * heads * rows * keys),
    )(scal, *kvs, *qs)


def diff_last(scal, kvs, state, mix_lambda, gain, rows, parts, chunks, offset):
    tiles = state[0].shape[0]
    heads = tiles // chunks
    size = rows // chunks
    others = list(range(1, parts))
    keys = rows * heads * len(others)
    return pl.pallas_call(
        functools.partial(diff_kernel, chunks, rows, heads, parts, others, offset),
        in_specs=[smem()] + [vmem()] * (len(kvs) + 3) + [smem()] * 2 + [vmem()],
        out_specs=[vmem()] * heads,
        out_shape=[jax.ShapeDtypeStruct((HEAD, size), jnp.bfloat16)] * heads,
        scratch_shapes=[
            pltpu.VMEM((1, HEAD + 16, 2 * size), jnp.float32),
            pltpu.VMEM((1, 1, 2 * size), jnp.float32),
            pltpu.VMEM((heads, HEAD, size), jnp.bfloat16),
            pltpu.VMEM((keys, 2 * HEAD), jnp.bfloat16),
            pltpu.VMEM((HEAD + 16, keys), jnp.bfloat16),
        ],
        compiler_params=pltpu.CompilerParams(vmem_limit_bytes=24 << 20),
        cost_estimate=cost(500 * heads * rows * keys),
    )(scal, *kvs, *state, mix_lambda, gain)


def out_kernel(heads, parts, offset, begin, scal_ref, win_ref, *refs):
    diff_refs = refs[:heads]
    win_w_ref, diff_w_ref, keep_ref, send_ref, stacked = refs[heads:]
    here, me = scal_ref[0] // parts, scal_ref[2]
    core = me % 2
    half = stacked.shape[1]
    win_width = win_ref.shape[1]

    @pl.when(pl.program_id(0) == 0)
    def _():
        for bit in range(2):
            at = pl.multiple_of((me ^ (2 * offset + bit)) * half, half)
            stacked[bit, :, 0:win_width] = win_ref[pl.ds(at, half), :]
        pieces = []
        for h in range(heads):
            piece = diff_refs[0][...]
            for d in range(1, heads):
                piece = jnp.where((here ^ d) == h, diff_refs[d][...], piece)
            pieces.append(piece)
        turned = jnp.transpose(jnp.concatenate(pieces, axis=0).astype(jnp.float32))
        turned = turned.astype(jnp.bfloat16)
        stacked[core, :, win_width:] = turned[0:half]
        stacked[1 - core, :, win_width:] = turned[half:]

    block = keep_ref.shape[1]
    at = pl.multiple_of(begin + pl.program_id(0) * block, block)
    lanes = pl.ds(at, block)
    weight = jnp.concatenate([win_w_ref[:, lanes], diff_w_ref[:, lanes]], axis=0)
    for i, ref in enumerate((keep_ref, send_ref)):
        ref[...] = jnp.dot(stacked[i], weight, preferred_element_type=jnp.float32).astype(
            jnp.bfloat16
        )


def out_part(scal, offset, win_rows, diffs, win_out, diff_out, begin, width, block, parts):
    heads = len(diffs)
    depth = win_out.shape[0] + diff_out.shape[0]
    size = diffs[0].shape[1]
    half = size // 2

    return pl.pallas_call(
        functools.partial(out_kernel, heads, parts, offset, begin),
        in_specs=[smem()] + [vmem()] * (3 + heads),
        out_specs=[pl.BlockSpec((half, block), lambda j: (0, j))] * 2,
        scratch_shapes=[pltpu.VMEM((2, half, depth), jnp.bfloat16)],
        grid=(width // block,),
        out_shape=[jax.ShapeDtypeStruct((half, width), jnp.bfloat16)] * 2,
        compiler_params=pltpu.CompilerParams(
            dimension_semantics=("arbitrary",), vmem_limit_bytes=16 << 20
        ),
        cost_estimate=cost(2 * size * depth * width),
    )(scal, win_rows, *diffs, win_out, diff_out)


def body(
    inputs,
    length,
    win_query,
    win_key,
    win_value,
    sink_logit,
    diff_query,
    diff_key,
    diff_value,
    mix_lambda,
    head_gain,
    win_out,
    diff_out,
):
    rows = inputs.shape[0]
    sp, tp = lax.axis_size("sp"), lax.axis_size("tp")
    chips = tp // 2
    size = rows // chips
    heads = mix_lambda.shape[0]
    parts = sp // heads
    here, me = lax.axis_index("sp"), lax.axis_index("tp")
    weights = (win_query, win_key, win_value, diff_query, diff_key, diff_value)
    scal = jnp.stack([here, length[0], me]).astype(jnp.int32)
    weights = fetch(weights, room=46 << 20)
    out_weights = fetch((win_out, diff_out), room=38 << 20)

    pieces = []
    for c in range(chips):
        pieces += fetch((inputs,), c * size, size, room=60 << 20)
    far = [
        [lax.ppermute(pieces[c], "tp", flip("tp", 2 * o)) for o in range(1, chips)]
        for c in range(chips)
    ]
    sib = lax.ppermute(inputs, "tp", flip("tp", 1))
    acc = project_near(inputs, sib, weights, scal)
    q_parts, kv_parts, own_kvs, other_kvs, qs = [], [], [], [], []
    for c in range(chips):
        xs = []
        for piece in far[c]:
            xs += [piece, lax.ppermute(piece, "tp", flip("tp", 1))]
        q_t, kv, *slots = project_far(acc, c, size, xs, weights, scal, heads, parts)
        q_parts.append(q_t)
        kv_parts.append(kv)
        moved = [slots[0]]
        for d in range(1, heads):
            moved.append(lax.ppermute(slots[d], "sp", flip("sp", d * parts)))
        mine = jnp.stack([m[:size] for m in moved])
        own_kvs.append(mine)
        other_kvs += [lax.ppermute(mine, "sp", flip("sp", e)) for e in range(1, parts)]
        qs += moved

    up = [(i, i + 1) for i in range(sp - 1)]
    down = [(i + 1, i) for i in range(sp - 1)]
    low = lax.ppermute(kv_parts[-1][size - WINDOW :], "sp", up)
    high = lax.ppermute(kv_parts[0][:WINDOW], "sp", down)
    edges = [low, *kv_parts, high]
    win_rows = []
    for c in range(chips):
        win_rows.append(
            window_part(scal, sink_logit, q_parts[c], *edges[c : c + 3], c * size, rows)
        )
    win_rows = jnp.concatenate(win_rows)

    gain = head_gain.reshape(1, HEAD)
    state = diff_first(scal, own_kvs, qs, rows, parts)

    def attend(o):
        return diff_last(
            scal, other_kvs, state, mix_lambda, gain, rows, parts, chips, o
        )

    def give_back(mixed):
        return [mixed[0]] + [
            lax.ppermute(mixed[d], "sp", flip("sp", d * parts)) for d in range(1, heads)
        ]

    mixed = [attend(o) for o in range(chips)]
    diffs = [give_back(mixed[o]) for o in range(chips)]

    width = win_out.shape[1]
    block = width // 4

    def project(o, begin, end):
        return out_part(
            scal, o, win_rows, diffs[o], *out_weights, begin, end - begin, block, parts
        )

    def add(*values):
        return functools.reduce(lambda a, b: a + b, [v.astype(jnp.float32) for v in values])

    cuts = (0, width // 4, width // 2, width)
    arrived = []
    for begin, end in zip(cuts[:-1], cuts[1:]):
        count = (end - begin) // block
        span = (end - begin) // count
        crossed = [[] for _ in range(count)]
        for o in range(1, chips):
            keep, away = project(o, begin, end)
            other = lax.ppermute(away, "tp", flip("tp", 1))
            pair = add(keep, other).astype(jnp.bfloat16)
            for i in range(count):
                piece = pair[:, i * span : (i + 1) * span]
                crossed[i].append(lax.ppermute(piece, "tp", flip("tp", 2 * o)))
        arrived += crossed
    outs = []
    for half in range(2):
        begin = half * (width // 2)
        keep, away = project(0, begin, begin + width // 2)
        other = lax.ppermute(away, "tp", flip("tp", 1))
        for i in range(2):
            lanes = slice(i * block, (i + 1) * block)
            crossed = arrived[2 * half + i]
            outs.append(add(keep[:, lanes], other[:, lanes], *crossed).astype(jnp.bfloat16))
    last = block
    early = jnp.concatenate(outs[:-1] + [keep[:, width // 2 - last :]], axis=1)
    early = lax.optimization_barrier(early)
    return lax.dynamic_update_slice(early, outs[-1], (0, width - last))


def solution(mesh):
    placed = (
        P("sp", "tp"),
        P(),
        P(None, "tp"),
        P(None, "tp"),
        P(None, "tp"),
        P("tp"),
        P(None, "tp"),
        P(None, "tp"),
        P(None, "tp"),
        P("tp"),
        P(),
        P("tp", None),
        P("tp", None),
    )

    return jax.shard_map(
        body, mesh=mesh, in_specs=placed, out_specs=P(("sp", "tp"), None), check_vma=False
    )
```

```python
import functools
import math

import jax
import jax.numpy as jnp
from jax import lax
from jax.experimental import pallas as pl
from jax.experimental.pallas import tpu as pltpu
from jax.sharding import PartitionSpec as P

HEAD = 64
DQK = 32
GROUP = 3
WINDOW = 128

epsilon = 1e-06
masked_score = -1e30
LOG2E = math.log2(math.e)
SAFE_BOUND = 90.0


def vmem():
    return pl.BlockSpec(memory_space=pltpu.VMEM)


def smem():
    return pl.BlockSpec(memory_space=pltpu.SMEM)


def cost(flops, bytes_accessed=0, transcendentals=0):
    return pl.CostEstimate(
        flops=flops, bytes_accessed=bytes_accessed, transcendentals=transcendentals
    )


def flip(axis, bits):
    return [(i, i ^ bits) for i in range(lax.axis_size(axis))]


def near_kernel(scal_ref, own_ref, sib_ref, *refs):
    weight_refs, acc_ref = refs[:-1], refs[-1]
    depth = own_ref.shape[1]
    me = scal_ref[2]
    low = 0
    for group in ((0, 1), (2, 3), (4,), (5,)):
        total = None
        for x_ref, k in ((own_ref, 0), (sib_ref, 1)):
            at = pl.multiple_of((me ^ k) * depth, depth)
            weight = jnp.concatenate([weight_refs[i][pl.ds(at, depth), :] for i in group], axis=1)
            added = jnp.dot(x_ref[...], weight, preferred_element_type=jnp.float32)
            total = added if total is None else total + added
        acc_ref[:, low : low + total.shape[1]] = total
        low += total.shape[1]


def project_near(own, sib, weights, scal):
    rows, depth = own.shape
    width = sum(w.shape[1] for w in weights)
    return pl.pallas_call(
        near_kernel,
        in_specs=[smem()] + [vmem()] * 8,
        out_specs=vmem(),
        out_shape=jax.ShapeDtypeStruct((rows, width), jnp.float32),
        compiler_params=pltpu.CompilerParams(vmem_limit_bytes=24 << 20),
        cost_estimate=cost(4 * rows * depth * width),
    )(scal, own, sib, *weights)


def copy_kernel(begin, *refs):
    count = len(refs) // 2
    sources, targets, semaphores = refs[:count], refs[count : 2 * count], refs[2 * count]
    copies = [
        pltpu.make_async_copy(
            source.at[pl.ds(begin, target.shape[0]), :], target, semaphores.at[i]
        )
        for i, (source, target) in enumerate(zip(sources, targets))
    ]
    for copy in copies:
        copy.start()
    for copy in copies:
        copy.wait()


def fetch(arrays, begin=0, rows=None, room=1 << 20):
    shapes = [(a.shape[0] if rows is None else rows, a.shape[1]) for a in arrays]
    return pl.pallas_call(
        functools.partial(copy_kernel, begin),
        in_specs=[pl.BlockSpec(memory_space=pltpu.HBM)] * len(arrays),
        out_specs=[pl.BlockSpec(memory_space=pltpu.VMEM)] * len(arrays),
        out_shape=[pltpu.VMEM(shape, jnp.bfloat16) for shape in shapes],
        scratch_shapes=[pltpu.SemaphoreType.DMA((len(arrays),))],
        compiler_params=pltpu.CompilerParams(vmem_limit_bytes=room),
        cost_estimate=cost(1 << 30),
    )(*arrays)


def far_kernel(begin, count, heads, parts, scal_ref, acc_ref, *refs):
    xs = refs[:count]
    weight_refs = refs[count : count + 6]
    qt_ref, kv_ref = refs[count + 6 : count + 8]
    slot_refs = refs[count + 8 : count + 8 + heads]
    buf_ref = refs[count + 8 + heads]
    rows, depth = xs[0].shape
    here = scal_ref[0] // parts

    def project(which):
        low = sum(weight_refs[i].shape[1] for i in range(which[0]))
        span = sum(weight_refs[i].shape[1] for i in which)
        total = acc_ref[begin : begin + rows, low : low + span]
        for n, x in enumerate(xs):
            at = pl.multiple_of((scal_ref[2] ^ (2 + n)) * depth, depth)
            weight = jnp.concatenate([weight_refs[i][pl.ds(at, depth), :] for i in which], axis=1)
            total += jnp.dot(x[...], weight, preferred_element_type=jnp.float32)
        ends = [sum(weight_refs[i].shape[1] for i in which[:n]) for n in range(len(which) + 1)]
        return [total[:, a:b] for a, b in zip(ends[:-1], ends[1:])]

    diff_k, diff_v = project((4, 5))
    win_v, diff_q = project((2, 3))
    win_q, win_k = project((0, 1))
    diff_q = diff_q * (LOG2E * DQK ** (-0.5))
    for h in range(heads):
        lanes = slice(h * HEAD, (h + 1) * HEAD)
        q, k, v = diff_q[:, lanes], diff_k[:, lanes], diff_v[:, lanes]
        buf_ref[h, 0:rows, :] = jnp.concatenate([k, v], axis=1).astype(jnp.bfloat16)
        pair = jnp.concatenate([q[: rows // 2], q[rows // 2 :]], axis=1)
        buf_ref[h, rows : rows + rows // 2, :] = pair.astype(jnp.bfloat16)
    for slot in range(heads):
        slot_refs[slot][...] = buf_ref[slot ^ here]
    qt_ref[...] = jnp.transpose(win_q * (LOG2E * HEAD ** (-0.5))).astype(jnp.bfloat16)
    kv_ref[...] = jnp.concatenate([win_k, win_v], axis=1).astype(jnp.bfloat16)


def project_far(acc, chunk, rows, xs, weights, scal, heads, parts):
    depth = xs[0].shape[1]
    count = len(xs)
    width = acc.shape[1]
    kv_width = weights[1].shape[1] + weights[2].shape[1]
    q_width = weights[0].shape[1]
    shapes = [(q_width, rows), (rows, kv_width)] + [(rows + rows // 2, 2 * HEAD)] * heads
    return pl.pallas_call(
        functools.partial(far_kernel, chunk * rows, count, heads, parts),
        in_specs=[smem()] + [vmem()] * (1 + count + 6),
        out_specs=[vmem() for shape in shapes],
        out_shape=[jax.ShapeDtypeStruct(shape, jnp.bfloat16) for shape in shapes],
        scratch_shapes=[pltpu.VMEM((heads, rows + rows // 2, 2 * HEAD), jnp.bfloat16)],
        compiler_params=pltpu.CompilerParams(vmem_limit_bytes=24 << 20),
        cost_estimate=cost(2 * count * rows * depth * width),
    )(scal, acc, *xs, *weights)


def window_kernel(begin, whole_rows, kv_local, scal_ref, sink_ref, *refs):
    q_ref, low_ref, kv_ref, high_ref, rows_ref, keys, values_t, out_ref = refs
    last = low_ref.shape[0] - WINDOW
    here, live = scal_ref[0], scal_ref[1]
    rows = kv_ref.shape[0]
    span = rows + 2 * WINDOW
    keys[0:WINDOW, :] = low_ref[last:, :]
    keys[WINDOW : WINDOW + rows, :] = kv_ref[...]
    keys[WINDOW + rows : span, :] = high_ref[0:WINDOW, :]
    k_width = kv_local * HEAD
    turned = jnp.transpose(keys[:, k_width:].astype(jnp.float32)).astype(jnp.bfloat16)
    tail = (lax.broadcasted_iota(jnp.int32, (16, span), 0) == 0).astype(jnp.bfloat16)
    for h in range(kv_local):
        values_t[h, 0:HEAD, :] = turned[h * HEAD : (h + 1) * HEAD]
        values_t[h, HEAD : HEAD + 16, :] = tail
    step = 128
    wide = step + 2 * WINDOW
    start = here * whole_rows + begin

    @pl.when(start >= live)
    def _():
        rows_ref[...] = jnp.zeros_like(rows_ref)

    @pl.when(start < live)
    def _():
        for b in range(rows // step):
            first, at = start + b * step, b * step
            key_at = lax.broadcasted_iota(jnp.int32, (wide, step), 0)
            gap = key_at - WINDOW - lax.broadcasted_iota(jnp.int32, (wide, step), 1)
            key_pos = first - WINDOW + key_at
            allowed = (gap <= WINDOW) & (gap >= -WINDOW) & (key_pos >= 0) & (key_pos < live)
            hidden = jnp.where(allowed, 0.0, masked_score)
            hidden = jnp.concatenate([hidden] * GROUP, axis=1)
            live_row = (first + lax.broadcasted_iota(jnp.int32, (1, step), 1)) < live
            for h in range(kv_local):
                key_block = keys[at : at + wide, h * HEAD : (h + 1) * HEAD]
                value_block = values_t[h, :, at : at + wide]
                members = range(h * GROUP, (h + 1) * GROUP)
                q = jnp.concatenate(
                    [q_ref[g * HEAD : (g + 1) * HEAD, at : at + step] for g in members], axis=1
                )
                sink = jnp.concatenate(
                    [jnp.full((1, step), sink_ref[g] * LOG2E, jnp.float32) for g in members], axis=1
                )
                s = jnp.dot(key_block, q, preferred_element_type=jnp.float32) + hidden
                top = jnp.maximum(jnp.max(s, axis=0, keepdims=True), sink)
                e = jnp.exp2(s - top).astype(jnp.bfloat16)
                mixed = jnp.dot(value_block, e, preferred_element_type=jnp.float32)
                total = mixed[HEAD : HEAD + 1] + jnp.exp2(sink - top)
                result = mixed[0:HEAD] / total
                for n, g in enumerate(members):
                    out_ref[g * HEAD : (g + 1) * HEAD, at : at + step] = jnp.where(
                        live_row, result[:, n * step : (n + 1) * step], 0.0
                    )
        rows_ref[...] = jnp.transpose(out_ref[...]).astype(jnp.bfloat16)


def window_part(scal, sink_logit, q_t, low, kv, high, begin, whole_rows):
    q_width, rows = q_t.shape
    kv_width = kv.shape[1]
    kv_local = kv_width // (2 * HEAD)
    return pl.pallas_call(
        functools.partial(window_kernel, begin, whole_rows, kv_local),
        in_specs=[smem()] * 2 + [vmem()] * 4,
        out_specs=vmem(),
        out_shape=jax.ShapeDtypeStruct((rows, q_width), jnp.bfloat16),
        scratch_shapes=[
            pltpu.VMEM((rows + 2 * WINDOW, kv_width), jnp.bfloat16),
            pltpu.VMEM((kv_local, HEAD + 16, rows + 2 * WINDOW), jnp.bfloat16),
            pltpu.VMEM((q_width, rows), jnp.float32),
        ],
        compiler_params=pltpu.CompilerParams(vmem_limit_bytes=16 << 20),
        cost_estimate=cost(40 * q_width * rows * 384),
    )(scal, sink_logit, q_t, low, kv, high)


def diff_kernel(chunks, rows, heads, parts, others, offset, scal_ref, *refs):
    first_call = offset is None
    kv_refs = refs[: chunks * len(others)]
    refs = refs[chunks * len(others) :]
    size = rows // chunks
    here, live = scal_ref[0], scal_ref[1]
    mine, part = here // parts, here % parts
    if first_call:
        q_refs, refs = refs[: chunks * heads], refs[chunks * heads :]
        queries, weighted, running, flags, keys, values_t = refs
    else:
        queries, weighted_in, running_in, flags, lam_ref, gain_ref = refs[:6]
        out_refs = refs[6 : 6 + heads]
        weighted, running, out_ref, keys, values_t = refs[6 + heads :]
        base = ((scal_ref[2] // 2) ^ offset) * heads
    step = 512
    pair = 2 * size
    total = keys.shape[0]

    live_keys = jnp.int32(0)
    for e in others:
        for h in range(heads):
            live_keys += jnp.clip(live - (h * parts + (part ^ e)) * rows, 0, rows)

    top_key = jnp.zeros((1, 2 * HEAD), jnp.float32)
    for n, e in enumerate(others):
        for c in range(chunks):
            for d in range(heads):
                owner, source = mine ^ d, part ^ e
                place = owner * len(others)
                if not first_call:
                    place += source - (source > part).astype(jnp.int32)
                at = pl.multiple_of(place * rows + c * size, size)
                block = kv_refs[c * len(others) + n][d]
                keys[pl.ds(at, size), :] = block
                wide = block.astype(jnp.float32)
                top_key = jnp.maximum(top_key, jnp.max(jnp.abs(wide), axis=0, keepdims=True))
                alive = (at + lax.broadcasted_iota(jnp.int32, (1, size), 1)) < live_keys
                turned = jnp.where(alive, jnp.transpose(wide)[HEAD:], 0.0)
                values_t[0:HEAD, pl.ds(at, size)] = turned.astype(jnp.bfloat16)
    counted = lax.broadcasted_iota(jnp.int32, (16, total), 0) == 0
    counted &= lax.broadcasted_iota(jnp.int32, (16, total), 1) < live_keys
    values_t[HEAD : HEAD + 16, :] = counted.astype(jnp.bfloat16)
    limit = jnp.transpose(jnp.broadcast_to(top_key, (8, 2 * HEAD)))[:, 0:1]
    if first_call:
        queries[...] = jnp.zeros_like(queries)
        for c in range(chunks):
            for d in range(heads):
                pairs = q_refs[c * heads + d][size : size + size // 2, :]
                turned = jnp.transpose(pairs.astype(jnp.float32))
                turned = jnp.concatenate([turned[0:HEAD], turned[HEAD:]], axis=1)
                turned = turned.astype(jnp.bfloat16)
                tile = c * heads + d
                queries[tile, 0:DQK, 0:size] = turned[0:DQK]
                queries[tile, DQK : 2 * DQK, size:pair] = turned[DQK:]
    else:
        gain = jnp.transpose(jnp.broadcast_to(gain_ref[...], (8, HEAD)))[:, 0:1]

    units = (live_keys + step - 1) // step

    def tile_body(index, carry):
        tile = index if first_call else base + index
        c, d = tile // heads, tile % heads
        first = (here ^ (d * parts)) * rows + c * size
        slot = tile if first_call else 0

        if first_call:
            flags[tile] = jnp.int32(0)
        else:

            @pl.when(first >= live)
            def _():
                out_ref[index] = jnp.zeros(out_ref.shape[1:], out_ref.dtype)

        @pl.when(first < live)
        def _():
            q = queries[tile]
            bound = jnp.max(jnp.sum(jnp.abs(q.astype(jnp.float32)) * limit, axis=0, keepdims=True))
            safe = bound < SAFE_BOUND
            if first_call:
                flags[tile] = safe.astype(jnp.int32)
                weighted[slot] = jnp.zeros(weighted.shape[1:], jnp.float32)
                running[slot] = jnp.where(
                    safe, jnp.zeros((1, pair), jnp.float32), masked_score
                )
            else:
                safe &= flags[tile] == 1
                weighted[slot] = weighted_in[tile]
                running[slot] = running_in[tile]

            def scores(j):
                at = pl.multiple_of(j * step, step)
                return jnp.dot(keys[pl.ds(at, step), :], q, preferred_element_type=jnp.float32)

            def values(j):
                return values_t[:, pl.ds(pl.multiple_of(j * step, step), step)]

            @pl.when(safe)
            def _():
                def several(j, number):
                    raised = [jnp.exp2(scores(j + i)).astype(jnp.bfloat16) for i in range(number)]
                    added = [
                        jnp.dot(values(j + i), e, preferred_element_type=jnp.float32)
                        for i, e in enumerate(raised)
                    ]
                    weighted[slot] += functools.reduce(lambda a, b: a + b, added)

                def one(j, carry):
                    several(4 * j, 4)
                    return carry

                lax.fori_loop(0, units // 4, one, 0)
                for number in (1, 2, 3):

                    @pl.when(units % 4 == number)
                    def _():
                        several(units - number, number)

            @pl.when(jnp.logical_not(safe))
            def _():
                def one(j, carry):
                    s = scores(j)
                    inside = lax.broadcasted_iota(jnp.int32, s.shape, 0) < live_keys - j * step
                    s = jnp.where(inside, s, masked_score)
                    old = running[slot]
                    new = jnp.maximum(old, jnp.max(s, axis=0, keepdims=True))
                    e = jnp.exp2(s - new).astype(jnp.bfloat16)
                    weighted[slot] = weighted[slot] * jnp.exp2(old - new) + jnp.dot(
                        values(j), e, preferred_element_type=jnp.float32
                    )
                    running[slot] = new
                    return carry

                lax.fori_loop(0, units, one, 0)

            if not first_call:
                maps = weighted[slot, 0:HEAD, :] / weighted[slot, HEAD : HEAD + 1, :]
                mix = maps[:, 0:size] - lam_ref[mine] * maps[:, size:pair]
                normed = mix * lax.rsqrt(jnp.mean(mix * mix, axis=0, keepdims=True) + epsilon)
                normed = normed * gain
                position = first + lax.broadcasted_iota(jnp.int32, (1, size), 1)
                out_ref[index] = jnp.where(position < live, normed, 0.0).astype(jnp.bfloat16)

        return carry

    lax.fori_loop(0, chunks * heads if first_call else heads, tile_body, 0)
    if not first_call:
        for d in range(heads):
            out_refs[d][...] = out_ref[d]


def diff_first(scal, kvs, qs, rows, parts):
    chunks = len(kvs)
    heads = len(qs) // chunks
    size = rows // chunks
    tiles = chunks * heads
    keys = rows * heads
    return pl.pallas_call(
        functools.partial(diff_kernel, chunks, rows, heads, parts, [0], None),
        in_specs=[smem()] + [vmem()] * (len(kvs) + len(qs)),
        out_specs=[vmem()] * 3 + [smem()],
        out_shape=[
            pltpu.VMEM((tiles, 2 * HEAD, 2 * size), jnp.bfloat16),
            pltpu.VMEM((tiles, HEAD + 16, 2 * size), jnp.float32),
            pltpu.VMEM((tiles, 1, 2 * size), jnp.float32),
            jax.ShapeDtypeStruct((tiles,), jnp.int32),
        ],
        scratch_shapes=[
            pltpu.VMEM((keys, 2 * HEAD), jnp.bfloat16),
            pltpu.VMEM((HEAD + 16, keys), jnp.bfloat16),
        ],
        compiler_params=pltpu.CompilerParams(vmem_limit_bytes=24 << 20),
        cost_estimate=cost(500 * heads * rows * keys),
    )(scal, *kvs, *qs)


def diff_last(scal, kvs, state, mix_lambda, gain, rows, parts, chunks, offset):
    tiles = state[0].shape[0]
    heads = tiles // chunks
    size = rows // chunks
    others = list(range(1, parts))
    keys = rows * heads * len(others)
    return pl.pallas_call(
        functools.partial(diff_kernel, chunks, rows, heads, parts, others, offset),
        in_specs=[smem()] + [vmem()] * (len(kvs) + 3) + [smem()] * 2 + [vmem()],
        out_specs=[vmem()] * heads,
        out_shape=[jax.ShapeDtypeStruct((HEAD, size), jnp.bfloat16)] * heads,
        scratch_shapes=[
            pltpu.VMEM((1, HEAD + 16, 2 * size), jnp.float32),
            pltpu.VMEM((1, 1, 2 * size), jnp.float32),
            pltpu.VMEM((heads, HEAD, size), jnp.bfloat16),
            pltpu.VMEM((keys, 2 * HEAD), jnp.bfloat16),
            pltpu.VMEM((HEAD + 16, keys), jnp.bfloat16),
        ],
        compiler_params=pltpu.CompilerParams(vmem_limit_bytes=24 << 20),
        cost_estimate=cost(500 * heads * rows * keys),
    )(scal, *kvs, *state, mix_lambda, gain)


def out_kernel(heads, parts, offset, begin, scal_ref, win_ref, *refs):
    diff_refs = refs[:heads]
    win_w_ref, diff_w_ref, keep_ref, send_ref, stacked = refs[heads:]
    here, me = scal_ref[0] // parts, scal_ref[2]
    core = me % 2
    half = stacked.shape[1]
    win_width = win_ref.shape[1]

    @pl.when(pl.program_id(0) == 0)
    def _():
        for bit in range(2):
            at = pl.multiple_of((me ^ (2 * offset + bit)) * half, half)
            stacked[bit, :, 0:win_width] = win_ref[pl.ds(at, half), :]
        pieces = []
        for h in range(heads):
            piece = diff_refs[0][...]
            for d in range(1, heads):
                piece = jnp.where((here ^ d) == h, diff_refs[d][...], piece)
            pieces.append(piece)
        turned = jnp.transpose(jnp.concatenate(pieces, axis=0).astype(jnp.float32))
        turned = turned.astype(jnp.bfloat16)
        stacked[core, :, win_width:] = turned[0:half]
        stacked[1 - core, :, win_width:] = turned[half:]

    block = keep_ref.shape[1]
    at = pl.multiple_of(begin + pl.program_id(0) * block, block)
    lanes = pl.ds(at, block)
    weight = jnp.concatenate([win_w_ref[:, lanes], diff_w_ref[:, lanes]], axis=0)
    for i, ref in enumerate((keep_ref, send_ref)):
        ref[...] = jnp.dot(stacked[i], weight, preferred_element_type=jnp.float32).astype(
            jnp.bfloat16
        )


def out_part(scal, offset, win_rows, diffs, win_out, diff_out, begin, width, block, parts):
    heads = len(diffs)
    depth = win_out.shape[0] + diff_out.shape[0]
    size = diffs[0].shape[1]
    half = size // 2

    return pl.pallas_call(
        functools.partial(out_kernel, heads, parts, offset, begin),
        in_specs=[smem()] + [vmem()] * (3 + heads),
        out_specs=[pl.BlockSpec((half, block), lambda j: (0, j))] * 2,
        scratch_shapes=[pltpu.VMEM((2, half, depth), jnp.bfloat16)],
        grid=(width // block,),
        out_shape=[jax.ShapeDtypeStruct((half, width), jnp.bfloat16)] * 2,
        compiler_params=pltpu.CompilerParams(
            dimension_semantics=("arbitrary",), vmem_limit_bytes=16 << 20
        ),
        cost_estimate=cost(2 * size * depth * width),
    )(scal, win_rows, *diffs, win_out, diff_out)


def body(
    inputs,
    length,
    win_query,
    win_key,
    win_value,
    sink_logit,
    diff_query,
    diff_key,
    diff_value,
    mix_lambda,
    head_gain,
    win_out,
    diff_out,
):
    rows = inputs.shape[0]
    sp, tp = lax.axis_size("sp"), lax.axis_size("tp")
    chips = tp // 2
    size = rows // chips
    heads = mix_lambda.shape[0]
    parts = sp // heads
    here, me = lax.axis_index("sp"), lax.axis_index("tp")
    weights = (win_query, win_key, win_value, diff_query, diff_key, diff_value)
    scal = jnp.stack([here, length[0], me]).astype(jnp.int32)
    weights = fetch(weights, room=46 << 20)
    out_weights = fetch((win_out, diff_out), room=38 << 20)

    pieces = []
    for c in range(chips):
        pieces += fetch((inputs,), c * size, size, room=60 << 20)
    far = [
        [lax.ppermute(pieces[c], "tp", flip("tp", 2 * o)) for o in range(1, chips)]
        for c in range(chips)
    ]
    sib = lax.ppermute(inputs, "tp", flip("tp", 1))
    acc = project_near(inputs, sib, weights, scal)
    q_parts, kv_parts, own_kvs, other_kvs, qs = [], [], [], [], []
    for c in range(chips):
        xs = []
        for piece in far[c]:
            xs += [piece, lax.ppermute(piece, "tp", flip("tp", 1))]
        q_t, kv, *slots = project_far(acc, c, size, xs, weights, scal, heads, parts)
        q_parts.append(q_t)
        kv_parts.append(kv)
        moved = [slots[0]]
        for d in range(1, heads):
            moved.append(lax.ppermute(slots[d], "sp", flip("sp", d * parts)))
        mine = jnp.stack([m[:size] for m in moved])
        own_kvs.append(mine)
        other_kvs += [lax.ppermute(mine, "sp", flip("sp", e)) for e in range(1, parts)]
        qs += moved

    up = [(i, i + 1) for i in range(sp - 1)]
    down = [(i + 1, i) for i in range(sp - 1)]
    low = lax.ppermute(kv_parts[-1][size - WINDOW :], "sp", up)
    high = lax.ppermute(kv_parts[0][:WINDOW], "sp", down)
    edges = [low, *kv_parts, high]
    win_rows = []
    for c in range(chips):
        win_rows.append(
            window_part(scal, sink_logit, q_parts[c], *edges[c : c + 3], c * size, rows)
        )
    win_rows = jnp.concatenate(win_rows)

    gain = head_gain.reshape(1, HEAD)
    state = diff_first(scal, own_kvs, qs, rows, parts)

    def attend(o):
        return diff_last(
            scal, other_kvs, state, mix_lambda, gain, rows, parts, chips, o
        )

    def give_back(mixed):
        return [mixed[0]] + [
            lax.ppermute(mixed[d], "sp", flip("sp", d * parts)) for d in range(1, heads)
        ]

    mixed = [attend(o) for o in range(chips)]
    diffs = [give_back(mixed[o]) for o in range(chips)]

    width = win_out.shape[1]
    block = width // 4

    def project(o, begin, end):
        return out_part(
            scal, o, win_rows, diffs[o], *out_weights, begin, end - begin, block, parts
        )

    def add(*values):
        return functools.reduce(lambda a, b: a + b, [v.astype(jnp.float32) for v in values])

    cuts = (0, width // 4, width // 2, width)
    arrived = []
    for begin, end in zip(cuts[:-1], cuts[1:]):
        count = (end - begin) // block
        span = (end - begin) // count
        crossed = [[] for _ in range(count)]
        for o in range(1, chips):
            keep, away = project(o, begin, end)
            other = lax.ppermute(away, "tp", flip("tp", 1))
            pair = add(keep, other).astype(jnp.bfloat16)
            for i in range(count):
                piece = pair[:, i * span : (i + 1) * span]
                crossed[i].append(lax.ppermute(piece, "tp", flip("tp", 2 * o)))
        arrived += crossed
    outs = []
    for half in range(2):
        begin = half * (width // 2)
        keep, away = project(0, begin, begin + width // 2)
        other = lax.ppermute(away, "tp", flip("tp", 1))
        for i in range(2):
            lanes = slice(i * block, (i + 1) * block)
            crossed = arrived[2 * half + i]
            outs.append(add(keep[:, lanes], other[:, lanes], *crossed).astype(jnp.bfloat16))
    last = block
    early = jnp.concatenate(outs[:-1] + [keep[:, width // 2 - last :]], axis=1)
    early = lax.optimization_barrier(early)
    return lax.dynamic_update_slice(early, outs[-1], (0, width - last))


def solution(mesh):
    placed = (
        P("sp", "tp"),
        P(),
        P(None, "tp"),
        P(None, "tp"),
        P(None, "tp"),
        P("tp"),
        P(None, "tp"),
        P(None, "tp"),
        P(None, "tp"),
        P("tp"),
        P(),
        P("tp", None),
        P("tp", None),
    )

    return jax.shard_map(
        body, mesh=mesh, in_specs=placed, out_specs=P(("sp", "tp"), None), check_vma=False
    )
```
